256 devices in a mesh: ep: 32 (over z, x), tp: 8 (over y, core).
Axes of the slice: x: 4, y: 4, z: 8, core: 2. Of those that a mesh axis runs over, the one named last changes fastest.
Arguments:
- queries: bfloat16 [16384, 1024], P('ep', 'tp'), may hold values from -8 to 8
- keys_values: bfloat16 [16384, 1024], P('ep', 'tp'), may hold values from -60 to 60
- forget_cache: float32 [16, 16384], P('tp'), may hold values from -2460 to 0, as said below
- heads_gain: float32 [1024], replicated, may hold values from 0.1 to 1.9
- output_weight: bfloat16 [1024, 2048], replicated, may hold values from -0.1875 to 0.1875
- expert_tokens: bfloat16 [4096, 2048], P('ep'), may hold values from -600 to 600
- expert_gain: float32 [2048], replicated, may hold values from 0.1 to 1.9
- routes: int32 [4096, 4], P('ep'), may hold values from 0 to 31, all different within a row; in each aligned block of 128 rows (0 to 127, 128 to 255, ...) at most 32 rows name the same one
- route_logits: float32 [4096, 4], P('ep'), may hold values from -6 to 301
- gate_weight: bfloat16 [32, 2048, 2048], P('ep', None, 'tp'), may hold values from -0.5 to 0.5
- up_weight: bfloat16 [32, 2048, 2048], P('ep', None, 'tp'), may hold values from -0.5 to 0.5
- down_weight: bfloat16 [32, 2048, 2048], P('ep', 'tp'), may hold values from -0.015625 to 0.015625
Outputs:
- mixer_out: bfloat16 [16384, 2048], P(('ep', 'tp'))
- moe_out: bfloat16 [4096, 2048], P('ep', 'tp')
The draws below stay inside these ranges and needn't reach their ends.
Inputs may be any that keep to these rules, and one draw needn't show every extreme that they name: `forget_cache`: each row never rises from one position to the next. `routes`: the 4 experts of a row differ. In each aligned block of 128 rows (one device's tokens) no expert is named more than 32 times, so slot is below 32; some expert is named exactly 32 times in some block.
All inputs are finite; a program needn't handle non-finite values.
Results may differ from the reference program's by a relative error of at most 0.017.
Values may be sent and summed in bfloat16 or wider, within the bound.
No kernel may reach another device: no remote copies, remote signals or barrier semaphores. Data moves between devices by JAX's collectives and lax.ppermute only.
A program may use at most 128 MiB of HBM per device.

```python
import math
import jax
import jax.numpy as jnp
import numpy as np
from jax import lax

D = 2048
ASKER_HEAD_TOTAL = 16
KV_HEADS = 8
HEAD = 64
FF = 2048
TOPK = 4
ATT_ROWS = 512
EXP_ROWS = 128
EXPERTS = 32
CAP = 32
MIXER_SEQ_SPAN = 16384
TOK_EXP = 4096
N_EP = 32
N_TP = 8


def base_values(key, shape):
    return jax.random.truncated_normal(key, -6.0, 6.0, shape, jnp.float32)


def draw_queries(key, part):
    result = base_values(jax.random.fold_in(key, 1), (MIXER_SEQ_SPAN, ASKER_HEAD_TOTAL, HEAD))
    return result.reshape(MIXER_SEQ_SPAN, ASKER_HEAD_TOTAL * HEAD).astype(jnp.bfloat16)


def draw_keys_values(key, part):
    key_rows = base_values(jax.random.fold_in(key, 2), (MIXER_SEQ_SPAN, KV_HEADS, HEAD))
    value_rows = base_values(jax.random.fold_in(key, 3), (MIXER_SEQ_SPAN, KV_HEADS, HEAD))
    scale_top = math.log(10.0)
    spread = jnp.exp(jax.random.uniform(jax.random.fold_in(key, 4), (1, KV_HEADS, HEAD), jnp.float32, 0.0, scale_top))
    value_rows = value_rows * spread
    joined = jnp.concatenate([key_rows, value_rows], axis=2)
    return joined.reshape(MIXER_SEQ_SPAN, KV_HEADS * 2 * HEAD).astype(jnp.bfloat16)


def draw_forget_cache(key, part):
    head_order = jax.random.permutation(jax.random.fold_in(key, 5), ASKER_HEAD_TOTAL)
    fast_heads = head_order < ASKER_HEAD_TOTAL // 2
    slow_rate = jnp.exp(jax.random.uniform(jax.random.fold_in(key, 6), (ASKER_HEAD_TOTAL,), jnp.float32, math.log(0.2), math.log(0.6))) / MIXER_SEQ_SPAN
    fast_rate = jnp.exp(jax.random.uniform(jax.random.fold_in(key, 7), (ASKER_HEAD_TOTAL,), jnp.float32, math.log(0.01), math.log(1.0 / 30.0)))
    step_rate = jnp.where(fast_heads, fast_rate, slow_rate)
    blocks = jnp.exp(jax.random.uniform(jax.random.fold_in(key, 8), (MIXER_SEQ_SPAN // ATT_ROWS,), jnp.float32, math.log(0.4), math.log(2.5)))
    per_block = jnp.repeat(blocks, ATT_ROWS)
    jitter = jax.random.uniform(jax.random.fold_in(key, 9), (ASKER_HEAD_TOTAL, MIXER_SEQ_SPAN), jnp.float32, 0.2, 1.8)
    decay_log_steps = step_rate[:, None] * per_block[None, :] * jitter
    decay_span_offset = jax.random.randint(jax.random.fold_in(key, 10), (ASKER_HEAD_TOTAL, 2), 0, MIXER_SEQ_SPAN)
    decay_span_size = jax.random.uniform(jax.random.fold_in(key, 12), (ASKER_HEAD_TOTAL, 2), jnp.float32, 0.22, 0.69)
    sequence_slot_number = jnp.arange(MIXER_SEQ_SPAN, dtype=jnp.int32)
    for decay_span_values in range(2):
        decay_log_steps = decay_log_steps + jnp.where(sequence_slot_number[None, :] == decay_span_offset[:, decay_span_values:decay_span_values + 1], decay_span_size[:, decay_span_values:decay_span_values + 1], 0.0)
    return -jnp.cumsum(decay_log_steps, axis=1)


def draw_expert_tokens(key, part):
    scale_top = math.log(10.0)
    result = base_values(jax.random.fold_in(key, 13), (TOK_EXP, D))
    row_scale = jnp.exp(jax.random.uniform(jax.random.fold_in(key, 14), (TOK_EXP, 1), jnp.float32, 0.0, math.log(10.0)))
    column_scale = jnp.exp(jax.random.uniform(jax.random.fold_in(key, 15), (1, D), jnp.float32, 0.0, scale_top))
    return (result * row_scale * column_scale).astype(jnp.bfloat16)


def draw_route_logits(key, part):
    result = base_values(jax.random.fold_in(key, 16), (TOK_EXP, TOPK))
    return result


def steps_of(stream_key, extent, shards, least, high):
    def one(dim, parts):
        heights = jax.random.uniform(jax.random.fold_in(jax.random.fold_in(stream_key, 6), dim), (parts,), jnp.float32, least / len(shards), high / len(shards))
        return jnp.repeat(jnp.exp(heights), extent[dim] // parts).reshape((-1,) + (1,) * (len(extent) - dim - 1))

    factor_of = one(*shards[0])
    for cut in shards[1:]:
        factor_of = factor_of * one(*cut)
    return factor_of


def deal_out(own_key, own, number, rows, count, top, limit, skew):
    sequence = jax.random.permutation(own_key, count)
    heavy_load, common = portions_of(count, rows * top, limit, skew, True), portions_of(count, rows * top, limit, skew, False)
    places = jnp.arange(count)

    def named(sizes, turn):
        used = int((sizes > 0).sum())
        fixed = max(1, used // 4)
        passed = fixed + (places - fixed + turn * (used - fixed)) % max(1, count - fixed)
        return jnp.zeros((count,), jnp.int32).at[sequence[jnp.where(places < fixed, places, passed)]].set(jnp.asarray(sizes, jnp.int32))

    sizes = jnp.where(number % 4 == 0, named(heavy_load, number // 4), named(common, number - number // 4 - 1))
    mixed = jax.random.permutation(jax.random.fold_in(own, 3), count)
    source_of, taker = mixed[0:count // 2 * 2:2], mixed[1:count // 2 * 2:2]
    slack = jnp.minimum(sizes[source_of] - 1, limit - sizes[taker]) // 2
    slack = jnp.where((source_of == sequence[0]) | (taker == sequence[0]) | (sizes[taker] == 0), 0, jnp.maximum(slack, 0))
    passed = jax.random.randint(jax.random.fold_in(own, 4), (count // 2,), 0, 1 << 20) % (slack + 1)
    sizes = sizes.at[source_of].add(-passed).at[taker].add(passed)
    items = jnp.searchsorted(jnp.cumsum(sizes), jnp.arange(rows * top), side="right").astype(jnp.int32)
    listing = items.reshape(top, rows).T
    listing = listing[jax.random.permutation(jax.random.fold_in(own, 1), rows)]
    turn = jax.random.randint(jax.random.fold_in(own, 2), (rows, 1), 0, top)
    return jnp.take_along_axis(listing, (jnp.arange(top)[None, :] + turn) % top, axis=1)


def portions_of(amount, total, bound, skew, full):
    portions = [(1 << 20) // math.isqrt(rank ** skew) + 1 for rank in range(1, amount + 1)]
    largest = bound if full else min(bound, max(-(-total // amount), total * portions[0] // sum(portions)))
    least = 1 if total - largest >= amount - 1 else 0
    given, surplus = [largest] + [least] * (amount - 1), total - largest - least * (amount - 1)
    while surplus > 0:
        movable = [i for i in range(1, amount) if given[i] < largest] or [i for i in range(1, amount) if given[i] < bound]
        whole, remaining = sum([portions[i] for i in movable]), surplus
        for i in movable:
            extra = min(bound - given[i], max(1, remaining * portions[i] // whole), surplus)
            given[i] = given[i] + extra
            surplus = surplus - extra
    return np.array(given)


def noise(own_key, dims, deviation, most, cuts=(), held_as=jnp.bfloat16):
    loudness = steps_of(own_key, dims, cuts, -0.22, 0.18) if cuts else 1.0
    values = jax.random.normal(own_key, dims, jnp.float32) * deviation * loudness
    return jnp.minimum(jnp.maximum(values, -most), most).astype(held_as)


def setup_inputs(seed: int = 0) -> dict:
    streams_of = jax.random.split(jax.random.key(seed), 13)
    queries = draw_queries(jax.random.fold_in(streams_of[12], 71), 0)
    keys_values = draw_keys_values(jax.random.fold_in(streams_of[12], 71), 0)
    forget_cache = draw_forget_cache(jax.random.fold_in(streams_of[12], 71), 0)
    heads_gain = jnp.clip(1.0 + 0.18 * jax.random.normal(streams_of[3], (ASKER_HEAD_TOTAL * HEAD,), jnp.float32), 0.1, 1.9)
    output_weight = noise(streams_of[4], (ASKER_HEAD_TOTAL * HEAD, D), (ASKER_HEAD_TOTAL * HEAD) ** -0.5, 0.1875)
    expert_tokens = draw_expert_tokens(jax.random.fold_in(streams_of[12], 71), 0)
    expert_gain = jnp.clip(1.0 + 0.18 * jax.random.normal(streams_of[6], (D,), jnp.float32), 0.1, 1.9)
    routes_keys = jax.random.split(jax.random.fold_in(streams_of[7], 1), TOK_EXP // EXP_ROWS)
    routes_turns = jax.random.permutation(jax.random.fold_in(streams_of[7], 3), TOK_EXP // EXP_ROWS)
    routes = jax.vmap(lambda own, number: deal_out(jax.random.fold_in(streams_of[7], 2), own, number, EXP_ROWS, EXPERTS, TOPK, CAP, 2))(routes_keys, routes_turns).reshape((TOK_EXP, TOPK))
    route_logits = draw_route_logits(jax.random.fold_in(streams_of[12], 71), 0)
    gate_weight = noise(streams_of[9], (EXPERTS, D, FF), (D // 16) ** -0.5, 0.5, ((0, 32), (2, 8)))
    up_weight = noise(streams_of[10], (EXPERTS, D, FF), (D // 16) ** -0.5, 0.5, ((0, 32), (2, 8)))
    down_weight = noise(streams_of[11], (EXPERTS, FF, D), (FF * 64) ** -0.5, 0.015625, ((0, 32), (1, 8)))
    return {"queries": queries, "keys_values": keys_values, "forget_cache": forget_cache, "heads_gain": heads_gain, "output_weight": output_weight, "expert_tokens": expert_tokens, "expert_gain": expert_gain, "routes": routes, "route_logits": route_logits, "gate_weight": gate_weight, "up_weight": up_weight, "down_weight": down_weight}


epsilon = 1e-06
clamp_limit = 7.0
sigmoid_slope = 1.702

def scaled_rows(values, gain_vector):
    as_float = values.astype(jnp.float32)
    inverse = lax.rsqrt(lax.optimization_barrier(jnp.mean(as_float * as_float, axis=-1, keepdims=True)) + epsilon)
    return (as_float * inverse * gain_vector.astype(jnp.float32)).astype(jnp.bfloat16)

def assign_slots(routes, experts, capacity):
    row_count, pick_count = routes.shape
    flat_routes = routes.reshape(-1)
    onehot = (flat_routes[:, None] == jnp.arange(experts, dtype=jnp.int32)[None, :]).astype(jnp.int32)
    earlier = jnp.cumsum(onehot, axis=0) - onehot
    slot_rank = lax.optimization_barrier(jnp.sum(earlier * onehot, axis=1)).astype(jnp.int32)
    position = (flat_routes * capacity + slot_rank).astype(jnp.int32)
    owner_row = (jnp.arange(row_count * pick_count, dtype=jnp.int32) // pick_count).astype(jnp.int32)
    slot_token = jnp.full((experts * capacity,), row_count, jnp.int32).at[position].set(owner_row)
    return (position.reshape(row_count, pick_count), slot_token)

def reference(queries, keys_values, forget_cache, heads_gain, output_weight, expert_tokens, expert_gain, routes, route_logits, gate_weight, up_weight, down_weight):
    group_size = ASKER_HEAD_TOTAL // KV_HEADS
    key_pairs = keys_values.reshape(MIXER_SEQ_SPAN, KV_HEADS, 2 * HEAD)
    query_heads = queries.reshape(MIXER_SEQ_SPAN, ASKER_HEAD_TOTAL, HEAD)
    block_width = math.gcd(MIXER_SEQ_SPAN, 512)
    key_pos = jnp.arange(MIXER_SEQ_SPAN, dtype=jnp.int32)
    score_scale = 1.0 / math.sqrt(HEAD)

    def one_head(head_number):
        key_head = head_number // group_size
        key_rows = key_pairs[:, key_head, :HEAD]
        value_rows = key_pairs[:, key_head, HEAD:]
        gate_row = forget_cache[head_number]
        query_all = query_heads[:, head_number, :]

        def one_block(block_index):
            first_row = block_index * block_width
            query_rows = lax.dynamic_slice_in_dim(query_all, first_row, block_width, 0)
            query_gate = lax.dynamic_slice_in_dim(gate_row, first_row, block_width, 0)
            scores = jnp.dot(query_rows, key_rows.T, preferred_element_type=jnp.float32) * score_scale
            scores = scores + query_gate[:, None] - gate_row[None, :]
            query_pos = first_row + jnp.arange(block_width, dtype=jnp.int32)
            scores = jnp.where(key_pos[None, :] <= query_pos[:, None], scores, -jnp.inf)
            row_max = lax.optimization_barrier(jnp.max(scores, axis=1, keepdims=True))
            weights = jnp.exp(scores - row_max)
            denominator = lax.optimization_barrier(jnp.sum(weights, axis=1, keepdims=True))
            summed = jnp.dot(weights.astype(jnp.bfloat16), value_rows, preferred_element_type=jnp.float32)
            return (summed / denominator).astype(jnp.bfloat16)
        return lax.map(one_block, jnp.arange(MIXER_SEQ_SPAN // block_width, dtype=jnp.int32)).reshape(MIXER_SEQ_SPAN, HEAD)
    attended = lax.map(one_head, jnp.arange(ASKER_HEAD_TOTAL, dtype=jnp.int32))
    attended = jnp.transpose(attended, (1, 0, 2)).reshape(MIXER_SEQ_SPAN, ASKER_HEAD_TOTAL * HEAD)
    heads_normed = scaled_rows(attended, heads_gain)
    mixer_out = jnp.dot(heads_normed, output_weight, preferred_element_type=jnp.float32).astype(jnp.bfloat16)
    expert_in = scaled_rows(expert_tokens, expert_gain)
    shifted = route_logits - lax.optimization_barrier(jnp.max(route_logits, axis=1, keepdims=True))
    raised = jnp.exp(shifted)
    route_weight = raised / lax.optimization_barrier(jnp.sum(raised, axis=1, keepdims=True))
    block_routes = routes.reshape(N_EP, EXP_ROWS, TOPK)
    block_weights = route_weight.reshape(N_EP, EXP_ROWS, TOPK)
    position, slot_token = jax.vmap(lambda chosen: assign_slots(chosen, EXPERTS, CAP))(block_routes)
    block_base = (jnp.arange(N_EP, dtype=jnp.int32) * EXP_ROWS)[:, None]
    global_token = jnp.where(slot_token < EXP_ROWS, slot_token + block_base, TOK_EXP).astype(jnp.int32)

    def weight_table(place, weights):
        return jnp.zeros((EXPERTS * CAP,), jnp.float32).at[place.reshape(-1)].set(weights.reshape(-1))
    slot_weight = jax.vmap(weight_table)(position, block_weights)
    padded = jnp.concatenate([expert_in, jnp.zeros((1, D), jnp.bfloat16)], axis=0)
    ff_block = FF // N_TP

    def accumulate(combined, expert):
        token_index = lax.dynamic_slice_in_dim(global_token, expert * CAP, CAP, 1).reshape(-1)
        slot_scale = lax.dynamic_slice_in_dim(slot_weight, expert * CAP, CAP, 1).reshape(-1)
        rows_in = jnp.take(padded, token_index, axis=0)
        gate_pre = jnp.dot(rows_in, gate_weight[expert], preferred_element_type=jnp.float32)
        up_pre = jnp.dot(rows_in, up_weight[expert], preferred_element_type=jnp.float32)
        gate_cut = jnp.minimum(gate_pre, clamp_limit)
        up_cut = jnp.clip(up_pre, -clamp_limit, clamp_limit)
        hidden = ((up_cut + 1.0) * gate_cut * jax.nn.sigmoid(sigmoid_slope * gate_cut)).astype(jnp.bfloat16)
        down_local = down_weight[expert]
        expert_sum = jnp.zeros((N_EP * CAP, D), jnp.float32)
        for block_index in range(N_TP):
            partial_value = jnp.dot(hidden[:, block_index * ff_block:(block_index + 1) * ff_block], down_local[block_index * ff_block:(block_index + 1) * ff_block, :], preferred_element_type=jnp.float32).astype(jnp.bfloat16)
            expert_sum = expert_sum + partial_value.astype(jnp.float32)
        expert_out = expert_sum.astype(jnp.bfloat16)
        combined = combined.at[token_index].add(expert_out.astype(jnp.float32) * slot_scale[:, None])
        return (combined, None)
    combined, _ = lax.scan(accumulate, jnp.zeros((TOK_EXP + 1, D), jnp.float32), jnp.arange(EXPERTS, dtype=jnp.int32))
    moe_out = combined[:TOK_EXP].astype(jnp.bfloat16)
    return (mixer_out, moe_out)
```

```python
import functools

import jax
import jax.numpy as jnp
from jax import lax
from jax.experimental import pallas as pl
from jax.experimental.pallas import tpu as pltpu
from jax.sharding import Mesh
from jax.sharding import PartitionSpec as P

EP = ("z", "x")
TP = ("y", "c")
epsilon = 1e-06
clamp_limit = 7.0
sigmoid_slope = 1.702


def scaled_rows(values, gain_vector):
    as_float = values.astype(jnp.float32)
    inverse = lax.rsqrt(jnp.mean(as_float * as_float, axis=-1, keepdims=True) + epsilon)
    return (as_float * inverse * gain_vector).astype(jnp.bfloat16)


BLK = 512
NEG = -1e30

def pieces_of(values):
    high = values.astype(jnp.bfloat16).astype(jnp.float32)
    rest = values - high
    middle = rest.astype(jnp.bfloat16).astype(jnp.float32)
    return high, middle, rest - middle

def attend_kernel(place, q_ref, kv_ref, fk_ref, fq_ref, o_ref, kaug, vaug, acc, top, knorm):
    step = pl.program_id(0)
    zed, ex = place[0], place[1]
    blocks = kv_ref.shape[0]

    @pl.when(step == 0)
    def _prepare():
        one = jnp.ones((blocks, BLK), jnp.float32)
        rows = [jnp.zeros((64, BLK), jnp.float32)]
        for h in range(2):
            rows += list(pieces_of(-fk_ref[h]))
        rows += [one, one]
        table = jnp.concatenate(rows, axis=0).T
        lane = lax.broadcasted_iota(jnp.int32, (BLK, 128), 1)
        tail = jnp.where(lax.broadcasted_iota(jnp.int32, (16, BLK), 0) == 0, 1.0, 0.0)
        most = jnp.zeros((1, BLK), jnp.float32)
        for b in range(blocks):
            block = kv_ref[b].astype(jnp.float32)
            kaug[b] = jnp.where(
                lane < 64, block, jnp.where((lane & 7) == b, table, 0.0)
            ).astype(jnp.bfloat16)
            turned = block.T
            vaug[b] = jnp.concatenate([turned[64:], tail], axis=0).astype(jnp.bfloat16)
            keys = turned[:64]
            most = jnp.maximum(most, jnp.sum(keys * keys, axis=0, keepdims=True))
        knorm[0] = jnp.max(most)

    q_turned = q_ref[0].astype(jnp.float32).T * 0.125
    q_most = jnp.maximum(
        jnp.max(jnp.sum(q_turned[:64] * q_turned[:64], axis=0, keepdims=True)),
        jnp.max(jnp.sum(q_turned[64:] * q_turned[64:], axis=0, keepdims=True)),
    )
    calm = q_most * knorm[0] <= 1600.0
    qaug = []
    for h in range(2):
        gate = fq_ref[0, h : h + 1]
        high, low, _ = pieces_of(gate)
        on, off = jnp.ones((24, BLK), jnp.float32), jnp.zeros((24, BLK), jnp.float32)
        qaug.append(
            jnp.concatenate(
                [
                    q_turned[64 * h : 64 * h + 64],
                    on if h == 0 else off,
                    on if h == 1 else off,
                    jnp.broadcast_to(high, (8, BLK)),
                    jnp.broadcast_to(low, (8, BLK)),
                ],
                axis=0,
            ).astype(jnp.bfloat16)
        )
    acc[...] = jnp.zeros_like(acc)
    full = zed + jnp.where(ex < step, 1, 0)
    half = BLK // 2

    def take(b, shifted, masked):
        for h in range(2):
            for part in range(2):
                span = slice(part * half, part * half + half)
                scores = jnp.dot(kaug[b], qaug[h][:, span], preferred_element_type=jnp.float32)
                if masked:
                    seen = lax.broadcasted_iota(jnp.int32, (BLK, half), 0) <= (
                        lax.broadcasted_iota(jnp.int32, (BLK, half), 1) + part * half
                    )
                    scores = jnp.where(seen, scores, NEG)
                if shifted:
                    old = top[h, :, span]
                    new = jnp.maximum(old, jnp.max(scores, axis=0, keepdims=True))
                    top[h, :, span] = new
                    acc[h, :, span] = acc[h, :, span] * jnp.exp(old - new)
                    scores = scores - new
                weights = jnp.exp(scores)
                if masked and shifted:
                    weights = jnp.where(seen, weights, 0.0)
                acc[h, :, span] += jnp.dot(
                    vaug[b], weights.astype(jnp.bfloat16), preferred_element_type=jnp.float32
                )

    def sweep(shifted):
        def one(b, carry):
            take(b, shifted, False)
            return carry

        lax.fori_loop(0, full, one, 0)

        @pl.when(ex == step)
        def _edge():
            take(zed, shifted, True)

    @pl.when(calm)
    def _calm():
        top[...] = jnp.zeros_like(top)
        sweep(False)

    @pl.when(jnp.logical_not(calm))
    def _wild():
        top[...] = jnp.full_like(top, NEG)
        sweep(True)

    for h in range(2):
        total = acc[h, 64:65]
        peak = top[h]
        rows = list(pieces_of(total)) + list(pieces_of(peak))
        rows.append(jnp.zeros((10, BLK), jnp.float32))
        o_ref[0, h] = jnp.concatenate([acc[h, :64]] + rows, axis=0).astype(jnp.bfloat16)

def attend(place, q4, kv8, fk, fq):
    n = kv8.shape[0]
    return pl.pallas_call(
        attend_kernel,
        grid_spec=pltpu.PrefetchScalarGridSpec(
            num_scalar_prefetch=1,
            grid=(4,),
            in_specs=[
                pl.BlockSpec((1, BLK, 128), lambda i, p: (i, 0, 0)),
                pl.BlockSpec((n, BLK, 128), lambda i, p: (0, 0, 0)),
                pl.BlockSpec((2, n, BLK), lambda i, p: (0, 0, 0)),
                pl.BlockSpec((1, 2, BLK), lambda i, p: (i, 0, 0)),
            ],
            out_specs=pl.BlockSpec((1, 2, 80, BLK), lambda i, p: (i, 0, 0, 0)),
            scratch_shapes=[
                pltpu.VMEM((n, BLK, 128), jnp.bfloat16),
                pltpu.VMEM((n, 80, BLK), jnp.bfloat16),
                pltpu.VMEM((2, 80, BLK), jnp.float32),
                pltpu.VMEM((2, 1, BLK), jnp.float32),
                pltpu.SMEM((1,), jnp.float32),
            ],
        ),
        out_shape=jax.ShapeDtypeStruct((4, 2, 80, BLK), jnp.bfloat16),
        name="attend",
    )(place, q4, kv8, fk, fq)

def merge_kernel(p_ref, o_ref):
    tops, sums, outs = [], [], []
    for h in range(2):
        peaks, totals = [], []
        for s in range(4):
            side = p_ref[s, h, 64:80].astype(jnp.float32)
            totals.append(side[0:1] + side[1:2] + side[2:3])
            peaks.append(side[3:4] + side[4:5] + side[5:6])
        peak = functools.reduce(jnp.maximum, peaks)
        factors = [jnp.exp(p - peak) for p in peaks]
        total = sum(f * t for f, t in zip(factors, totals))
        value = sum(f * p_ref[s, h, :64].astype(jnp.float32) for s, f in enumerate(factors))
        outs.append(value / total)
    o_ref[...] = jnp.concatenate(outs, axis=0).T.astype(jnp.bfloat16)

def merge(parts):
    return pl.pallas_call(
        merge_kernel,
        out_shape=jax.ShapeDtypeStruct((BLK, 128), jnp.bfloat16),
        name="merge",
    )(parts)

def shift(array, axis, by):
    count = lax.axis_size(axis)
    return lax.ppermute(array, axis, [(i, (i + by) % count) for i in range(count)])


def spread(array, axis):
    count = lax.axis_size(axis)
    return lax.all_to_all(
        jnp.broadcast_to(array[None], (count, *array.shape)), axis, 0, 0, tiled=True
    )


def hidden_kernel(order, *refs):
    pieces, (gate_ref, up_ref, out_ref) = refs[:8], refs[8:]
    gate = up = None
    for n, piece in enumerate(pieces):
        rows = pl.ds(pl.multiple_of(order[n] * 256, 256), 256)
        left = piece[...]
        g = jnp.dot(left, gate_ref[rows, :], preferred_element_type=jnp.float32)
        u = jnp.dot(left, up_ref[rows, :], preferred_element_type=jnp.float32)
        gate, up = (g, u) if n == 0 else (gate + g, up + u)
    gate = jnp.minimum(gate, clamp_limit)
    up = jnp.clip(up, -clamp_limit, clamp_limit)
    out_ref[...] = ((up + 1.0) * gate * jax.nn.sigmoid(sigmoid_slope * gate)).astype(jnp.bfloat16)


def hidden_of(order, pieces, gate_local, up_local):
    rows = pieces[0].shape[0]
    tile = 256
    return pl.pallas_call(
        hidden_kernel,
        grid_spec=pltpu.PrefetchScalarGridSpec(
            num_scalar_prefetch=1,
            grid=(rows // tile,),
            in_specs=[pl.BlockSpec((tile, 256), lambda i, o: (i, 0))] * 8
            + [pl.BlockSpec((2048, 256), lambda i, o: (0, 0))] * 2,
            out_specs=pl.BlockSpec((tile, 256), lambda i, o: (i, 0)),
        ),
        out_shape=jax.ShapeDtypeStruct((rows, 256), jnp.bfloat16),
        name="hidden",
    )(order, *pieces, gate_local, up_local)


def body(
    queries,
    keys_values,
    forget_cache,
    heads_gain,
    output_weight,
    expert_tokens,
    expert_gain,
    routes,
    route_logits,
    gate_weight,
    up_weight,
    down_weight,
):
    zed, ex = lax.axis_index("z"), lax.axis_index("x")
    why, core = lax.axis_index("y"), lax.axis_index("c")
    rank = lax.axis_index(TP)
    rows = routes.shape[0]
    experts, capacity, width = 32, 32, 256

    tokens = expert_tokens.astype(jnp.float32)
    inverse = lax.rsqrt(jnp.mean(tokens * tokens, axis=-1, keepdims=True) + epsilon)
    own = lax.dynamic_slice_in_dim(tokens, rank * width, width, 1)
    own_gain = lax.dynamic_slice_in_dim(expert_gain, rank * width, width, 0)
    own_in = (own * inverse * own_gain).astype(jnp.bfloat16)

    chosen = routes.T[None, :, :] == jnp.arange(experts, dtype=jnp.int32)[:, None, None]
    named = jnp.any(chosen, axis=1)
    number = jnp.arange(rows, dtype=jnp.int32)
    earlier = (number[:, None] < number[None, :]).astype(jnp.bfloat16)
    slot = jnp.dot(named.astype(jnp.bfloat16), earlier, preferred_element_type=jnp.float32)
    slot = jnp.where(named, slot.astype(jnp.int32), -1)
    place = slot[:, None, :] == jnp.arange(capacity, dtype=jnp.int32)[None, :, None]
    onehot = place.astype(jnp.bfloat16).reshape(experts * capacity, rows)
    outgoing = jnp.dot(onehot, own_in, preferred_element_type=jnp.float32).astype(jnp.bfloat16)
    arrived = lax.all_to_all(
        outgoing.reshape(experts, capacity, width), EP, 0, 0, tiled=True
    ).reshape(experts * capacity, width)

    kv, q, arrived = lax.optimization_barrier((keys_values, queries, arrived))
    pieces = [arrived] + [shift(arrived, "y", by) for by in (1, 3, 2)]
    places = [2 * ((why - by) % 4) for by in (0, 1, 3, 2)]
    twins = [shift(piece, "c", 1) for piece in pieces]
    order = jnp.stack([p + core for p in places] + [p + 1 - core for p in places]).astype(jnp.int32)

    kv8 = spread(kv, "z")
    q4 = spread(q, "x")
    gates = forget_cache.reshape(2, 8, 4, BLK)
    fk = lax.dynamic_index_in_dim(gates, ex, 2, keepdims=False)
    fq = lax.dynamic_index_in_dim(gates, zed, 1, keepdims=False).transpose(1, 0, 2)

    hidden = hidden_of(order, pieces + twins, gate_weight[0], up_weight[0])
    down = down_weight[0].reshape(width, 4, 2, width)

    def partial(by, side):
        part = lax.dynamic_slice(
            down, (0, (why + by) % 4, side, 0), (width, 1, 1, width)
        ).reshape(width, width)
        return jnp.dot(hidden, part, preferred_element_type=jnp.float32)

    steps = (2, 1, 3, 0)
    others = [shift(partial(by, 1 - core).astype(jnp.bfloat16), "c", 1) for by in steps]
    pairs = [
        (partial(by, core) + other.astype(jnp.float32)).astype(jnp.bfloat16)
        for by, other in zip(steps, others)
    ]
    moved = [shift(pair, "y", by) if by else pair for by, pair in zip(steps, pairs)]
    expert_out = sum(m.astype(jnp.float32) for m in moved).astype(jnp.bfloat16)

    parts = attend(jnp.stack([zed, ex]).astype(jnp.int32), q4, kv8, fk, fq)
    parts = lax.all_to_all(parts, "x", 0, 0, tiled=True)
    attended = merge(parts)
    local = lax.all_to_all(attended, TP, split_axis=0, concat_axis=1, tiled=True)

    returned = lax.all_to_all(
        expert_out.reshape(experts, capacity, width), EP, 0, 0, tiled=True
    ).reshape(experts * capacity, width)

    heads_normed = scaled_rows(local, heads_gain)
    mixer_out = jnp.dot(heads_normed, output_weight, preferred_element_type=jnp.float32).astype(
        jnp.bfloat16
    )

    shifted = route_logits - jnp.max(route_logits, axis=1, keepdims=True)
    raised = jnp.exp(shifted)
    route_weight = raised / jnp.sum(raised, axis=1, keepdims=True)
    share = jnp.sum(jnp.where(chosen, route_weight.T[None, :, :], 0.0), axis=1)
    high = share.astype(jnp.bfloat16)
    low = (share - high.astype(jnp.float32)).astype(jnp.bfloat16)
    moe = 0.0
    for piece in (high, low):
        table = jnp.where(place, piece[:, None, :], jnp.bfloat16(0)).reshape(-1, rows)
        moe = moe + lax.dot_general(
            table, returned, (((0,), (0,)), ((), ())), preferred_element_type=jnp.float32
        )
    return (mixer_out, moe.astype(jnp.bfloat16))


def solution(mesh):
    torus = Mesh(mesh.devices.reshape(8, 4, 4, 2), ("z", "x", "y", "c"))
    return jax.shard_map(
        body,
        mesh=torus,
        in_specs=(
            P(EP, TP),
            P(EP, TP),
            P(TP, None),
            P(),
            P(),
            P(EP, None),
            P(),
            P(EP, None),
            P(EP, None),
            P(EP, None, TP),
            P(EP, None, TP),
            P(EP, TP, None),
        ),
        out_specs=(P(EP + TP, None), P(EP, TP)),
        check_vma=False,
    )
```

```python
import functools

import jax
import jax.numpy as jnp
from jax import lax
from jax.experimental import pallas as pl
from jax.experimental.pallas import tpu as pltpu
from jax.sharding import Mesh
from jax.sharding import PartitionSpec as P


EP = ("z", "x")
TP = ("y", "c")
epsilon = 1e-06
clamp_limit = 7.0
sigmoid_slope = 1.702


BLK = 512
NEG = -1e30


def pieces_of(values):
    high = values.astype(jnp.bfloat16).astype(jnp.float32)
    rest = values - high
    middle = rest.astype(jnp.bfloat16).astype(jnp.float32)
    return high, middle, rest - middle


def attend_kernel(place, q_ref, kv_ref, fk_ref, fq_ref, o_ref, kaug, vaug, qaug, held, acc, top, knorm):
    step = pl.program_id(0)
    zed, ex = place[0], place[1]
    blocks = kv_ref.shape[0]
    half = BLK // 2

    @pl.when(step == 0)
    def _prepare():
        one = jnp.ones((blocks, BLK), jnp.float32)
        rows = [jnp.zeros((64, BLK), jnp.float32)]
        for h in range(2):
            rows += list(pieces_of(-fk_ref[h]))
        rows += [one, one]
        table = jnp.concatenate(rows, axis=0).T
        lane = lax.broadcasted_iota(jnp.int32, (BLK, 128), 1)
        tail = jnp.where(lax.broadcasted_iota(jnp.int32, (16, BLK), 0) == 0, 1.0, 0.0)
        most = jnp.zeros((1, BLK), jnp.float32)
        for b in range(blocks):
            block = kv_ref[b].astype(jnp.float32)
            kaug[b] = jnp.where(
                lane < 64, block, jnp.where((lane & 7) == b, table, 0.0)
            ).astype(jnp.bfloat16)
            turned = block.T
            vaug[b] = jnp.concatenate([turned[64:], tail], axis=0).astype(jnp.bfloat16)
            keys = turned[:64]
            most = jnp.maximum(most, jnp.sum(keys * keys, axis=0, keepdims=True))
        knorm[0] = jnp.max(most)

    q_turned = q_ref[0].astype(jnp.float32).T * 0.125
    q_most = jnp.maximum(
        jnp.max(jnp.sum(q_turned[:64] * q_turned[:64], axis=0, keepdims=True)),
        jnp.max(jnp.sum(q_turned[64:] * q_turned[64:], axis=0, keepdims=True)),
    )
    calm = q_most * knorm[0] <= 1600.0
    for h in range(2):
        gate = fq_ref[0, h : h + 1]
        high, low, _ = pieces_of(gate)
        on, off = jnp.ones((24, BLK), jnp.float32), jnp.zeros((24, BLK), jnp.float32)
        whole = jnp.concatenate(
            [
                q_turned[64 * h : 64 * h + 64],
                on if h == 0 else off,
                on if h == 1 else off,
                jnp.broadcast_to(high, (8, BLK)),
                jnp.broadcast_to(low, (8, BLK)),
            ],
            axis=0,
        ).astype(jnp.bfloat16)
        for part in range(2):
            qaug[part, h] = whole[:, part * half : part * half + half]
    acc[...] = jnp.zeros_like(acc)
    home = (ex - step) & 3
    after = jnp.where(ex < home, 1, 0)
    low_count = zed + after
    count = blocks - 1 + 2 * after

    def unit(i):
        first = i < low_count
        return jnp.where(first, 0, 1), jnp.where(first, i, i - low_count)

    def scores_of(part, b, h):
        return jnp.dot(kaug[b], qaug[part, h], preferred_element_type=jnp.float32)

    def add(part, b, h, weights):
        acc[part, h] += jnp.dot(
            vaug[b], weights.astype(jnp.bfloat16), preferred_element_type=jnp.float32
        )

    def shifted_add(part, b, h, scores, seen):
        old = top[part, h]
        new = jnp.maximum(old, jnp.max(scores, axis=0, keepdims=True))
        top[part, h] = new
        acc[part, h] = acc[part, h] * jnp.exp(old - new)
        weights = jnp.exp(scores - new)
        add(part, b, h, weights if seen is None else jnp.where(seen, weights, 0.0))

    def seen_of(part):
        return lax.broadcasted_iota(jnp.int32, (BLK, half), 0) <= (
            lax.broadcasted_iota(jnp.int32, (BLK, half), 1) + part * half
        )

    @pl.when(calm)
    def _calm():
        top[...] = jnp.zeros_like(top)
        part, b = unit(0)
        for h in range(2):
            held[h] = scores_of(part, b, h)

        def one(i, carry):
            part, b = unit(i)
            next_part, next_b = unit(jnp.minimum(i + 1, count - 1))
            for h in range(2):
                weights = jnp.exp(held[h])
                held[h] = scores_of(next_part, next_b, h)
                add(part, b, h, weights)
            return carry

        lax.fori_loop(0, count, one, 0)

        @pl.when(step == 0)
        def _edge():
            for part, b in ((0, zed), (1, blocks - 1 - zed)):
                for h in range(2):
                    add(part, b, h, jnp.exp(jnp.where(seen_of(part), scores_of(part, b, h), NEG)))

    @pl.when(jnp.logical_not(calm))
    def _wild():
        top[...] = jnp.full_like(top, NEG)

        def one(i, carry):
            part, b = unit(i)
            for h in range(2):
                shifted_add(part, b, h, scores_of(part, b, h), None)
            return carry

        lax.fori_loop(0, count, one, 0)

        @pl.when(step == 0)
        def _edge():
            for part, b in ((0, zed), (1, blocks - 1 - zed)):
                for h in range(2):
                    seen = seen_of(part)
                    scores = jnp.where(seen, scores_of(part, b, h), NEG)
                    shifted_add(part, b, h, scores, seen)

    for h in range(2):
        for part in range(2):
            rows = list(pieces_of(acc[part, h, 64:65])) + list(pieces_of(top[part, h]))
            rows.append(jnp.zeros((10, half), jnp.float32))
            o_ref[0, h, :, part * half : part * half + half] = jnp.concatenate(
                [acc[part, h, :64]] + rows, axis=0
            ).astype(jnp.bfloat16)


def attend(place, q4, kv8, fk, fq):
    n = kv8.shape[0]
    half = BLK // 2
    return pl.pallas_call(
        attend_kernel,
        grid_spec=pltpu.PrefetchScalarGridSpec(
            num_scalar_prefetch=1,
            grid=(4,),
            in_specs=[
                pl.BlockSpec((1, BLK, 128), lambda i, p: (i, 0, 0)),
                pl.BlockSpec((n, BLK, 128), lambda i, p: (0, 0, 0)),
                pl.BlockSpec((2, n, BLK), lambda i, p: (0, 0, 0)),
                pl.BlockSpec((1, 2, BLK), lambda i, p: ((p[1] - i) & 3, 0, 0)),
            ],
            out_specs=pl.BlockSpec((1, 2, 80, BLK), lambda i, p: (i, 0, 0, 0)),
            scratch_shapes=[
                pltpu.VMEM((n, BLK, 128), jnp.bfloat16),
                pltpu.VMEM((n, 80, BLK), jnp.bfloat16),
                pltpu.VMEM((2, 2, 128, half), jnp.bfloat16),
                pltpu.VMEM((2, BLK, half), jnp.float32),
                pltpu.VMEM((2, 2, 80, half), jnp.float32),
                pltpu.VMEM((2, 2, 1, half), jnp.float32),
                pltpu.SMEM((1,), jnp.float32),
            ],
        ),
        out_shape=jax.ShapeDtypeStruct((4, 2, 80, BLK), jnp.bfloat16),
        name="attend",
    )(place, q4, kv8, fk, fq)


def merge_kernel(*refs):
    parts, o_ref = refs[:4], refs[4]
    outs = []
    for h in range(2):
        peaks, totals = [], []
        for part in parts:
            side = part[h, 64:80].astype(jnp.float32)
            totals.append(side[0:1] + side[1:2] + side[2:3])
            peaks.append(side[3:4] + side[4:5] + side[5:6])
        peak = functools.reduce(jnp.maximum, peaks)
        factors = [jnp.exp(p - peak) for p in peaks]
        total = sum(f * t for f, t in zip(factors, totals))
        value = sum(f * part[h, :64].astype(jnp.float32) for part, f in zip(parts, factors))
        outs.append(value / total)
    o_ref[...] = jnp.concatenate(outs, axis=0).T.astype(jnp.bfloat16)


def merge(parts):
    return pl.pallas_call(
        merge_kernel,
        out_shape=jax.ShapeDtypeStruct((BLK, 128), jnp.bfloat16),
        name="merge",
    )(*parts)


def project_kernel(order, *refs):
    pieces, (gain_ref, weight_ref, out_ref) = refs[:4], refs[4:]
    lefts = [piece[s].astype(jnp.float32) for piece in pieces for s in range(2)]
    squares = sum(jnp.sum(left * left, axis=1, keepdims=True) for left in lefts)
    inverse = lax.rsqrt(squares * (1.0 / 1024.0) + epsilon)
    total = None
    for n, left in enumerate(lefts):
        normed = (left * inverse * gain_ref[pl.ds(order[n], 1), :]).astype(jnp.bfloat16)
        rows = pl.ds(pl.multiple_of(order[n] * 128, 128), 128)
        term = jnp.dot(normed, weight_ref[rows, :], preferred_element_type=jnp.float32)
        total = term if n == 0 else total + term
    out_ref[...] = total.astype(jnp.bfloat16)


def project(order, pieces, gain, weight):
    vmem = pl.BlockSpec(memory_space=pltpu.VMEM)
    return pl.pallas_call(
        project_kernel,
        in_specs=[pl.BlockSpec(memory_space=pltpu.SMEM)] + [vmem] * 6,
        out_specs=vmem,
        out_shape=jax.ShapeDtypeStruct((64, 2048), jnp.bfloat16),
        name="project",
    )(order, *pieces, gain.reshape(8, 128), weight)


def shift(array, axis, by):
    count = lax.axis_size(axis)
    return lax.ppermute(array, axis, [(i, (i + by) % count) for i in range(count)])


def mirror(array):
    count = lax.axis_size("z")
    return lax.ppermute(array, "z", [(i, count - 1 - i) for i in range(count)])


def spread(array, axis):
    count = lax.axis_size(axis)
    return lax.all_to_all(
        jnp.broadcast_to(array[None], (count, *array.shape)), axis, 0, 0, tiled=True
    )


def hidden_kernel(order, *refs):
    pieces, (gate_ref, up_ref, out_ref) = refs[:10], refs[10:]
    upper = pl.program_id(0) < pl.num_programs(0) // 2
    lefts = [piece[...] for piece in pieces[:6]]
    lefts += [jnp.where(upper, a[...], b[...]) for a, b in (pieces[6:8], pieces[8:])]
    gate = up = None
    for n, left in enumerate(lefts):
        rows = pl.ds(pl.multiple_of(order[n] * 256, 256), 256)
        g = jnp.dot(left, gate_ref[rows, :], preferred_element_type=jnp.float32)
        u = jnp.dot(left, up_ref[rows, :], preferred_element_type=jnp.float32)
        gate, up = (g, u) if n == 0 else (gate + g, up + u)
    gate = jnp.minimum(gate, clamp_limit)
    up = jnp.clip(up, -clamp_limit, clamp_limit)
    out_ref[...] = ((up + 1.0) * gate * jax.nn.sigmoid(sigmoid_slope * gate)).astype(jnp.bfloat16)


def hidden_of(order, pieces, gate_local, up_local):
    rows = pieces[0].shape[0]
    tile = 256
    half = rows // tile // 2
    whole = pl.BlockSpec((tile, 256), lambda i, o: (i, 0))
    upper = pl.BlockSpec((tile, 256), lambda i, o: (jnp.minimum(i, half - 1), 0))
    lower = pl.BlockSpec((tile, 256), lambda i, o: (jnp.maximum(i - half, 0), 0))
    return pl.pallas_call(
        hidden_kernel,
        grid_spec=pltpu.PrefetchScalarGridSpec(
            num_scalar_prefetch=1,
            grid=(rows // tile,),
            in_specs=[whole] * 6
            + [upper, lower] * 2
            + [pl.BlockSpec((2048, 256), lambda i, o: (0, 0))] * 2,
            out_specs=whole,
        ),
        out_shape=jax.ShapeDtypeStruct((rows, 256), jnp.bfloat16),
        name="hidden",
    )(order, *pieces, gate_local, up_local)


def body(
    queries,
    keys_values,
    forget_cache,
    heads_gain,
    output_weight,
    expert_tokens,
    expert_gain,
    routes,
    route_logits,
    gate_weight,
    up_weight,
    down_weight,
):
    zed, ex = lax.axis_index("z"), lax.axis_index("x")
    why, core = lax.axis_index("y"), lax.axis_index("c")
    rank = lax.axis_index(TP)
    rows = routes.shape[0]
    experts, capacity, width = 32, 32, 256

    middle = BLK // 2
    q = jnp.concatenate([queries[:middle], mirror(queries[middle:])], axis=0)
    q4 = jnp.stack([q] + [shift(q, "x", by) for by in (1, 2, 3)])

    tokens = expert_tokens.astype(jnp.float32)
    inverse = lax.rsqrt(jnp.mean(tokens * tokens, axis=-1, keepdims=True) + epsilon)
    own = lax.dynamic_slice_in_dim(tokens, rank * width, width, 1)
    own_gain = lax.dynamic_slice_in_dim(expert_gain, rank * width, width, 0)
    own_in = (own * inverse * own_gain).astype(jnp.bfloat16)

    chosen = routes.T[None, :, :] == jnp.arange(experts, dtype=jnp.int32)[:, None, None]
    named = jnp.any(chosen, axis=1)
    number = jnp.arange(rows, dtype=jnp.int32)
    earlier = (number[:, None] < number[None, :]).astype(jnp.bfloat16)
    slot = jnp.dot(named.astype(jnp.bfloat16), earlier, preferred_element_type=jnp.float32)
    slot = jnp.where(named, slot.astype(jnp.int32), -1)
    place = slot[:, None, :] == jnp.arange(capacity, dtype=jnp.int32)[None, :, None]
    onehot = place.astype(jnp.bfloat16).reshape(experts * capacity, rows)
    outgoing = jnp.dot(onehot, own_in, preferred_element_type=jnp.float32).astype(jnp.bfloat16)
    arrived = lax.all_to_all(
        outgoing.reshape(experts, capacity, width), EP, 0, 0, tiled=True
    ).reshape(experts * capacity, width)

    kv, arrived = lax.optimization_barrier((keys_values, arrived))
    near = experts * capacity // 2
    left, right = shift(arrived, "y", 1), shift(arrived, "y", 3)
    far = [shift(left[:near], "y", 1), shift(right[near:], "y", 3)]
    pieces = [arrived, left, right]
    pieces += [shift(piece, "c", 1) for piece in pieces]
    pieces += far + [shift(piece, "c", 1) for piece in far]
    places = [2 * ((why - by) % 4) for by in (0, 1, 3)]
    order = [p + core for p in places] + [p + 1 - core for p in places]
    last = 2 * ((why + 2) % 4)
    order = jnp.stack(order + [last + core, last + 1 - core]).astype(jnp.int32)

    kv8 = spread(kv, "z")
    gates = forget_cache.reshape(2, 8, 4, BLK)
    fk = lax.dynamic_index_in_dim(gates, ex, 2, keepdims=False)
    fq = jnp.concatenate(
        [
            lax.dynamic_index_in_dim(gates, zed, 1, keepdims=False)[:, :, :middle],
            lax.dynamic_index_in_dim(gates, 7 - zed, 1, keepdims=False)[:, :, middle:],
        ],
        axis=2,
    ).transpose(1, 0, 2)

    hidden = hidden_of(order, pieces, gate_weight[0], up_weight[0])
    down = down_weight[0].reshape(width, 4, 2, width)

    def partial(by, side):
        part = lax.dynamic_slice(
            down, (0, (why + by) % 4, side, 0), (width, 1, 1, width)
        ).reshape(width, width)
        return jnp.dot(hidden, part, preferred_element_type=jnp.float32)

    steps = (2, 1, 3, 0)
    others = [shift(partial(by, 1 - core).astype(jnp.bfloat16), "c", 1) for by in steps]
    pairs = [
        (partial(by, core) + other.astype(jnp.float32)).astype(jnp.bfloat16)
        for by, other in zip(steps, others)
    ]
    far, after, before, kept = [pair for pair in pairs]
    first, second = shift(far[:near], "y", 1), shift(far[near:], "y", 3)

    def joined(pair, extra, top):
        total = (pair[:near] if top else pair[near:]).astype(jnp.float32) + extra.astype(jnp.float32)
        total = total.astype(jnp.bfloat16)
        return jnp.concatenate([total, pair[near:]] if top else [pair[:near], total], axis=0)

    moved = [kept, shift(joined(after, first, True), "y", 1)]
    moved.append(shift(joined(before, second, False), "y", 3))
    expert_out = sum(m.astype(jnp.float32) for m in moved).astype(jnp.bfloat16)

    parts = attend(jnp.stack([zed, ex]).astype(jnp.int32), q4, kv8, fk, fq)
    parts = [parts[0]] + [shift(parts[by], "x", 4 - by) for by in (1, 2, 3)]
    returned = lax.all_to_all(
        expert_out.reshape(experts, capacity, width), EP, 0, 0, tiled=True
    ).reshape(experts * capacity, width)
    attended = merge(parts)
    attended = jnp.concatenate([attended[:middle], mirror(attended[middle:])], axis=0)
    attended = attended.reshape(4, 2, 64, 128)
    twin = shift(lax.dynamic_index_in_dim(attended, 1 - core, 1, keepdims=False), "c", 1)
    mine = lax.dynamic_index_in_dim(attended, core, 1, keepdims=False)
    both = jnp.stack([mine, twin], axis=1)
    slices = []
    for by in range(4):
        piece = lax.dynamic_index_in_dim(both, (why + by) % 4, 0, keepdims=False)
        slices.append(shift(piece, "y", by) if by else piece)
    heads = [2 * ((why - by) % 4) + side for by in range(4) for side in (core, 1 - core)]
    mixer_out = project(jnp.stack(heads).astype(jnp.int32), slices, heads_gain, output_weight)

    shifted = route_logits - jnp.max(route_logits, axis=1, keepdims=True)
    raised = jnp.exp(shifted)
    route_weight = raised / jnp.sum(raised, axis=1, keepdims=True)
    share = jnp.sum(jnp.where(chosen, route_weight.T[None, :, :], 0.0), axis=1)
    high = share.astype(jnp.bfloat16)
    low = (share - high.astype(jnp.float32)).astype(jnp.bfloat16)
    moe = 0.0
    for piece in (high, low):
        table = jnp.where(place, piece[:, None, :], jnp.bfloat16(0)).reshape(-1, rows)
        moe = moe + lax.dot_general(
            table, returned, (((0,), (0,)), ((), ())), preferred_element_type=jnp.float32
        )
    return (mixer_out, moe.astype(jnp.bfloat16))


def solution(mesh):
    torus = Mesh(mesh.devices.reshape(8, 4, 4, 2), ("z", "x", "y", "c"))
    return jax.shard_map(
        body,
        mesh=torus,
        in_specs=(
            P(EP, TP),
            P(EP, TP),
            P(TP, None),
            P(),
            P(),
            P(EP, None),
            P(),
            P(EP, None),
            P(EP, None),
            P(EP, None, TP),
            P(EP, None, TP),
            P(EP, TP, None),
        ),
        out_specs=(P(EP + TP, None), P(EP, TP)),
        check_vma=False,
    )
```

```python
import functools

import jax
import jax.numpy as jnp
from jax import lax
from jax.experimental import pallas as pl
from jax.experimental.pallas import tpu as pltpu
from jax.sharding import Mesh
from jax.sharding import PartitionSpec as P


EP = ("z", "x")
TP = ("y", "c")
epsilon = 1e-06
clamp_limit = 7.0
sigmoid_slope = 1.702


BLK = 512
NEG = -1e30
KEYS_FROM = (0, 7, 1, 6, 2, 5, 3, 4)


def pieces_of(values):
    high = values.astype(jnp.bfloat16).astype(jnp.float32)
    rest = values - high
    middle = rest.astype(jnp.bfloat16).astype(jnp.float32)
    return high, middle, rest - middle


def attend_kernel(first, place, *refs):
    q_refs, kv_refs = refs[:2], refs[2:10]
    fk_ref, low_ref, high_ref, o_ref, kaug, vaug, qaug, held, acc, top, knorm = refs[10:]
    turn = pl.program_id(0)
    step = turn + first
    zed, ex = place[0], place[1]
    blocks = len(kv_refs)
    half = BLK // 2

    @pl.when(turn == 0)
    def _prepare():
        one = jnp.ones((blocks, BLK), jnp.float32)
        rows = [jnp.zeros((64, BLK), jnp.float32)]
        for h in range(2):
            rows += list(pieces_of(-fk_ref[h, :, 0, 0, :]))
        rows += [one, one]
        table = jnp.concatenate(rows, axis=0).T
        lane = lax.broadcasted_iota(jnp.int32, (BLK, 128), 1)
        tail = jnp.where(lax.broadcasted_iota(jnp.int32, (16, BLK), 0) == 0, 1.0, 0.0)
        most = jnp.zeros((1, BLK), jnp.float32)
        for kv_ref, away in zip(kv_refs, KEYS_FROM):
            b = (zed + away) & 7
            block = kv_ref[...].astype(jnp.float32)
            kaug[b] = jnp.where(
                lane < 64, block, jnp.where((lane & 7) == b, table, 0.0)
            ).astype(jnp.bfloat16)
            turned = block.T
            vaug[b] = jnp.concatenate([turned[64:], tail], axis=0).astype(jnp.bfloat16)
            keys = turned[:64]
            most = jnp.maximum(most, jnp.sum(keys * keys, axis=0, keepdims=True))
        knorm[0] = jnp.max(most)

    q_now = jnp.where(turn == 0, q_refs[0][...], q_refs[1][...])
    q_turned = q_now.astype(jnp.float32).T * 0.125
    q_most = jnp.maximum(
        jnp.max(jnp.sum(q_turned[:64] * q_turned[:64], axis=0, keepdims=True)),
        jnp.max(jnp.sum(q_turned[64:] * q_turned[64:], axis=0, keepdims=True)),
    )
    calm = q_most * knorm[0] <= 1600.0
    for h in range(2):
        gate = jnp.concatenate(
            [low_ref[h, 0, 0, :, :half], high_ref[h, 0, 0, :, half:]], axis=1
        )
        high, low, _ = pieces_of(gate)
        on, off = jnp.ones((24, BLK), jnp.float32), jnp.zeros((24, BLK), jnp.float32)
        whole = jnp.concatenate(
            [
                q_turned[64 * h : 64 * h + 64],
                on if h == 0 else off,
                on if h == 1 else off,
                jnp.broadcast_to(high, (8, BLK)),
                jnp.broadcast_to(low, (8, BLK)),
            ],
            axis=0,
        ).astype(jnp.bfloat16)
        for part in range(2):
            qaug[part, h] = whole[:, part * half : part * half + half]
    acc[...] = jnp.zeros_like(acc)
    home = (ex - step) & 3
    after = jnp.where(ex < home, 1, 0)
    low_count = zed + after
    count = blocks - 1 + 2 * after

    def unit(i):
        first = i < low_count
        return jnp.where(first, 0, 1), jnp.where(first, i, i - low_count)

    def scores_of(part, b, h):
        return jnp.dot(kaug[b], qaug[part, h], preferred_element_type=jnp.float32)

    def add(part, b, h, weights):
        acc[part, h] += jnp.dot(
            vaug[b], weights.astype(jnp.bfloat16), preferred_element_type=jnp.float32
        )

    def seen_of(part):
        return lax.broadcasted_iota(jnp.int32, (BLK, half), 0) <= (
            lax.broadcasted_iota(jnp.int32, (BLK, half), 1) + part * half
        )

    @pl.when(calm)
    def _calm():
        top[...] = jnp.zeros_like(top)
        part, b = unit(0)
        for h in range(2):
            held[h] = scores_of(part, b, h)

        def one(i, carry):
            part, b = unit(i)
            next_part, next_b = unit(jnp.minimum(i + 1, count - 1))
            for h in range(2):
                weights = jnp.exp(held[h])
                held[h] = scores_of(next_part, next_b, h)
                add(part, b, h, weights)
            return carry

        lax.fori_loop(0, count, one, 0)

        def edge(part):
            b = jnp.where(part == 0, zed, blocks - 1 - zed)
            for h in range(2):
                add(part, b, h, jnp.exp(jnp.where(seen_of(part), scores_of(part, b, h), NEG)))

        if first == 0:
            lax.fori_loop(0, jnp.where(turn == 0, 2, 0), lambda part, c: (edge(part), c)[1], 0)

    @pl.when(jnp.logical_not(calm))
    def _wild():
        top[...] = jnp.full_like(top, NEG)
        low_all = zed + jnp.where(ex <= home, 1, 0)

        def one(i, carry):
            h, n = i & 1, i >> 1
            part = jnp.where(n < low_all, 0, 1)
            b = n - part * low_all
            edge = (step == 0) & (b == jnp.where(part == 0, zed, blocks - 1 - zed))
            seen = seen_of(part + jnp.where(edge, 0, 4))
            scores = jnp.where(seen, scores_of(part, b, h), NEG)
            old = top[part, h]
            new = jnp.maximum(old, jnp.max(scores, axis=0, keepdims=True))
            top[part, h] = new
            acc[part, h] = acc[part, h] * jnp.exp(old - new)
            add(part, b, h, jnp.where(seen, jnp.exp(scores - new), 0.0))
            return carry

        lax.fori_loop(0, 2 * (blocks - 1 + 2 * jnp.where(ex <= home, 1, 0)), one, 0)

    for h in range(2):
        for part in range(2):
            rows = list(pieces_of(acc[part, h, 64:65])) + list(pieces_of(top[part, h]))
            rows.append(jnp.zeros((10, half), jnp.float32))
            o_ref[0, h, :, part * half : part * half + half] = jnp.concatenate(
                [acc[part, h, :64]] + rows, axis=0
            ).astype(jnp.bfloat16)


def attend(first, place, q_pair, kv_list, gates):
    n = len(kv_list)
    half = BLK // 2
    whole = pl.BlockSpec((BLK, 128), lambda i, p: (0, 0))
    one_gate = (2, 1, 1, 1, BLK)
    return pl.pallas_call(
        functools.partial(attend_kernel, first),
        grid_spec=pltpu.PrefetchScalarGridSpec(
            num_scalar_prefetch=1,
            grid=(2,),
            in_specs=[whole] * (2 + n)
            + [
                pl.BlockSpec((2, n, 1, 1, BLK), lambda i, p: (0, 0, p[1], 0, 0)),
                pl.BlockSpec(one_gate, lambda i, p: (0, p[0], (p[1] - i - first) & 3, 0, 0)),
                pl.BlockSpec(one_gate, lambda i, p: (0, 7 - p[0], (p[1] - i - first) & 3, 0, 0)),
            ],
            out_specs=pl.BlockSpec((1, 2, 80, BLK), lambda i, p: (i, 0, 0, 0)),
            scratch_shapes=[
                pltpu.VMEM((n, BLK, 128), jnp.bfloat16),
                pltpu.VMEM((n, 80, BLK), jnp.bfloat16),
                pltpu.VMEM((2, 2, 128, half), jnp.bfloat16),
                pltpu.VMEM((2, BLK, half), jnp.float32),
                pltpu.VMEM((2, 2, 80, half), jnp.float32),
                pltpu.VMEM((2, 2, 1, half), jnp.float32),
                pltpu.SMEM((1,), jnp.float32),
            ],
        ),
        out_shape=jax.ShapeDtypeStruct((2, 2, 80, BLK), jnp.bfloat16),
        name="attend",
    )(place, *q_pair, *kv_list, gates, gates, gates)


def merge_kernel(*refs):
    parts, o_ref = refs[:4], refs[4]
    outs = []
    for h in range(2):
        peaks, totals = [], []
        for part in parts:
            side = part[h, 64:80].astype(jnp.float32)
            totals.append(side[0:1] + side[1:2] + side[2:3])
            peaks.append(side[3:4] + side[4:5] + side[5:6])
        peak = functools.reduce(jnp.maximum, peaks)
        factors = [jnp.exp(p - peak) for p in peaks]
        total = sum(f * t for f, t in zip(factors, totals))
        value = sum(f * part[h, :64].astype(jnp.float32) for part, f in zip(parts, factors))
        outs.append(value / total)
    o_ref[...] = jnp.concatenate(outs, axis=0).T.astype(jnp.bfloat16)


def merge(parts):
    return pl.pallas_call(
        merge_kernel,
        out_shape=jax.ShapeDtypeStruct((BLK, 128), jnp.bfloat16),
        name="merge",
    )(*parts)


def project_kernel(order, *refs):
    pieces, (gain_ref, weight_ref, out_ref) = refs[:4], refs[4:]
    lefts = [piece[s].astype(jnp.float32) for piece in pieces for s in range(2)]
    squares = sum(jnp.sum(left * left, axis=1, keepdims=True) for left in lefts)
    inverse = lax.rsqrt(squares * (1.0 / 1024.0) + epsilon)
    total = None
    for n, left in enumerate(lefts):
        normed = (left * inverse * gain_ref[pl.ds(order[n], 1), :]).astype(jnp.bfloat16)
        rows = pl.ds(pl.multiple_of(order[n] * 128, 128), 128)
        term = jnp.dot(normed, weight_ref[rows, :], preferred_element_type=jnp.float32)
        total = term if n == 0 else total + term
    out_ref[...] = total.astype(jnp.bfloat16)


def project(order, pieces, gain, weight):
    vmem = pl.BlockSpec(memory_space=pltpu.VMEM)
    return pl.pallas_call(
        project_kernel,
        in_specs=[pl.BlockSpec(memory_space=pltpu.SMEM)] + [vmem] * 6,
        out_specs=vmem,
        out_shape=jax.ShapeDtypeStruct((64, 2048), jnp.bfloat16),
        name="project",
    )(order, *pieces, gain.reshape(8, 128), weight)


def shift(array, axis, by):
    count = lax.axis_size(axis)
    return lax.ppermute(array, axis, [(i, (i + by) % count) for i in range(count)])


def mirror(array):
    count = lax.axis_size("z")
    return lax.ppermute(array, "z", [(i, count - 1 - i) for i in range(count)])


def hidden_kernel(order, *refs):
    pieces, (gate_ref, up_ref, out_ref) = refs[:10], refs[10:]
    upper = pl.program_id(0) < pl.num_programs(0) // 2
    lefts = [piece[...] for piece in pieces[:6]]
    lefts += [jnp.where(upper, a[...], b[...]) for a, b in (pieces[6:8], pieces[8:])]
    gate = up = None
    for n, left in enumerate(lefts):
        rows = pl.ds(pl.multiple_of(order[n] * 256, 256), 256)
        g = jnp.dot(left, gate_ref[rows, :], preferred_element_type=jnp.float32)
        u = jnp.dot(left, up_ref[rows, :], preferred_element_type=jnp.float32)
        gate, up = (g, u) if n == 0 else (gate + g, up + u)
    gate = jnp.minimum(gate, clamp_limit)
    up = jnp.clip(up, -clamp_limit, clamp_limit)
    out_ref[...] = ((up + 1.0) * gate * jax.nn.sigmoid(sigmoid_slope * gate)).astype(jnp.bfloat16)


def hidden_of(order, pieces, gate_local, up_local):
    rows = pieces[0].shape[0]
    tile = 256
    half = rows // tile // 2
    whole = pl.BlockSpec((tile, 256), lambda i, o: (i, 0))
    upper = pl.BlockSpec((tile, 256), lambda i, o: (jnp.minimum(i, half - 1), 0))
    lower = pl.BlockSpec((tile, 256), lambda i, o: (jnp.maximum(i - half, 0), 0))
    return pl.pallas_call(
        hidden_kernel,
        grid_spec=pltpu.PrefetchScalarGridSpec(
            num_scalar_prefetch=1,
            grid=(rows // tile,),
            in_specs=[whole] * 6
            + [upper, lower] * 2
            + [pl.BlockSpec((2048, 256), lambda i, o: (0, 0))] * 2,
            out_specs=whole,
        ),
        out_shape=jax.ShapeDtypeStruct((rows, 256), jnp.bfloat16),
        name="hidden",
    )(order, *pieces, gate_local, up_local)


def body(
    queries,
    keys_values,
    forget_cache,
    heads_gain,
    output_weight,
    expert_tokens,
    expert_gain,
    routes,
    route_logits,
    gate_weight,
    up_weight,
    down_weight,
):
    zed, ex = lax.axis_index("z"), lax.axis_index("x")
    why, core = lax.axis_index("y"), lax.axis_index("c")
    rank = lax.axis_index(TP)
    rows = routes.shape[0]
    experts, capacity, width = 32, 32, 256

    middle = BLK // 2
    turned = mirror(queries[middle:])
    q = jnp.concatenate([queries[:middle], turned], axis=0)
    q_list = [q] + [shift(q, "x", by) for by in (1, 2, 3)]
    ups, downs = [keys_values], [keys_values]
    for _ in range(3):
        ups.append(shift(ups[-1], "z", 1))
    for _ in range(4):
        downs.append(shift(downs[-1], "z", 7))
    kv_list = [keys_values, ups[1], downs[1], ups[2], downs[2], ups[3], downs[3], downs[4]]

    tokens = expert_tokens.astype(jnp.float32)
    inverse = lax.rsqrt(jnp.mean(tokens * tokens, axis=-1, keepdims=True) + epsilon)
    own = lax.dynamic_slice_in_dim(expert_tokens, rank * width, width, 1).astype(jnp.float32)
    own_gain = lax.dynamic_slice_in_dim(expert_gain, rank * width, width, 0)
    own_in = (own * inverse * own_gain).astype(jnp.bfloat16)

    chosen = routes.T[None, :, :] == jnp.arange(experts, dtype=jnp.int32)[:, None, None]
    named = jnp.any(chosen, axis=1)
    number = jnp.arange(rows, dtype=jnp.int32)
    earlier = (number[:, None] < number[None, :]).astype(jnp.bfloat16)
    slot = jnp.dot(named.astype(jnp.bfloat16), earlier, preferred_element_type=jnp.float32)
    slot = jnp.where(named, slot.astype(jnp.int32), -1)
    place = slot[:, None, :] == jnp.arange(capacity, dtype=jnp.int32)[None, :, None]
    onehot = place.astype(jnp.bfloat16).reshape(experts * capacity, rows)
    outgoing = jnp.dot(onehot, own_in, preferred_element_type=jnp.float32).astype(jnp.bfloat16)
    arrived = lax.all_to_all(
        outgoing.reshape(experts, capacity, width), EP, 0, 0, tiled=True
    ).reshape(experts * capacity, width)
    near = experts * capacity // 2
    left, right = shift(arrived, "y", 1), shift(arrived, "y", 3)
    far = [shift(left[:near], "y", 1), shift(right[near:], "y", 3)]
    pieces = [arrived, left, right]
    pieces += [shift(piece, "c", 1) for piece in pieces]
    pieces += far + [shift(piece, "c", 1) for piece in far]
    ways = jnp.array([0, 1, 3, 0, 1, 3, 2, 2], jnp.int32)
    sides = jnp.array([0, 0, 0, 1, 1, 1, 0, 1], jnp.int32)
    order = 2 * ((why - ways) & 3) + (core ^ sides)

    hidden = hidden_of(order, pieces, gate_weight[0], up_weight[0])
    down = down_weight[0].reshape(width, 4, 2, width)

    def partial(by, side):
        part = lax.dynamic_slice(
            down, (0, (why + by) & 3, side, 0), (width, 1, 1, width)
        ).reshape(width, width)
        return jnp.dot(hidden, part, preferred_element_type=jnp.float32)

    steps = (2, 1, 3, 0)
    others = [shift(partial(by, 1 - core).astype(jnp.bfloat16), "c", 1) for by in steps]
    pairs = [
        (partial(by, core) + other.astype(jnp.float32)).astype(jnp.bfloat16)
        for by, other in zip(steps, others)
    ]
    far, after, before, kept = [pair for pair in pairs]
    first, second = shift(far[:near], "y", 1), shift(far[near:], "y", 3)

    def joined(pair, extra, top):
        total = (pair[:near] if top else pair[near:]).astype(jnp.float32) + extra.astype(jnp.float32)
        total = total.astype(jnp.bfloat16)
        return jnp.concatenate([total, pair[near:]] if top else [pair[:near], total], axis=0)

    moved = [kept, shift(joined(after, first, True), "y", 1)]
    moved.append(shift(joined(before, second, False), "y", 3))
    expert_out = sum(m.astype(jnp.float32) for m in moved).astype(jnp.bfloat16)

    gates = forget_cache.reshape(2, 8, 4, 1, BLK)
    spot = jnp.stack([zed, ex]).astype(jnp.int32)
    parts = attend(0, spot, q_list[:2], kv_list, gates)
    parts = [parts[0], shift(parts[1], "x", 3)]
    rest = attend(2, spot, q_list[2:], kv_list, gates)
    parts += [shift(rest[0], "x", 2), shift(rest[1], "x", 1)]
    returned = lax.all_to_all(
        expert_out.reshape(experts, capacity, width), EP, 0, 0, tiled=True
    ).reshape(experts * capacity, width)
    attended = merge(parts)
    turned = mirror(attended[middle:])
    attended = jnp.concatenate([attended[:middle], turned], axis=0)
    attended = attended.reshape(4, 2, 64, 128)
    twin = shift(lax.dynamic_index_in_dim(attended, 1 - core, 1, keepdims=False), "c", 1)
    mine = lax.dynamic_index_in_dim(attended, core, 1, keepdims=False)
    both = jnp.stack([mine, twin], axis=1)
    slices = []
    for by in range(4):
        piece = lax.dynamic_index_in_dim(both, (why + by) & 3, 0, keepdims=False)
        slices.append(shift(piece, "y", by) if by else piece)
    ways = jnp.array([0, 0, 1, 1, 2, 2, 3, 3], jnp.int32)
    sides = jnp.array([0, 1, 0, 1, 0, 1, 0, 1], jnp.int32)
    heads = 2 * ((why - ways) & 3) + (core ^ sides)
    mixer_out = project(heads, slices, heads_gain, output_weight)

    shifted = route_logits - jnp.max(route_logits, axis=1, keepdims=True)
    raised = jnp.exp(shifted)
    route_weight = raised / jnp.sum(raised, axis=1, keepdims=True)
    share = jnp.sum(jnp.where(chosen, route_weight.T[None, :, :], 0.0), axis=1)
    high = share.astype(jnp.bfloat16)
    low = (share - high.astype(jnp.float32)).astype(jnp.bfloat16)
    moe = 0.0
    for piece in (high, low):
        table = jnp.where(place, piece[:, None, :], jnp.bfloat16(0)).reshape(-1, rows)
        moe = moe + lax.dot_general(
            table, returned, (((0,), (0,)), ((), ())), preferred_element_type=jnp.float32
        )
    return (mixer_out, moe.astype(jnp.bfloat16))


def solution(mesh):
    torus = Mesh(mesh.devices.reshape(8, 4, 4, 2), ("z", "x", "y", "c"))
    return jax.shard_map(
        body,
        mesh=torus,
        in_specs=(
            P(EP, TP),
            P(EP, TP),
            P(TP, None),
            P(),
            P(),
            P(EP, None),
            P(),
            P(EP, None),
            P(EP, None),
            P(EP, None, TP),
            P(EP, None, TP),
            P(EP, TP, None),
        ),
        out_specs=(P(EP + TP, None), P(EP, TP)),
        check_vma=False,
    )
```

```python
import functools

import jax
import jax.numpy as jnp
from jax import lax
from jax.experimental import pallas as pl
from jax.experimental.pallas import tpu as pltpu
from jax.sharding import Mesh
from jax.sharding import PartitionSpec as P


EP = ("z", "x")
TP = ("y", "c")
epsilon = 1e-06
clamp_limit = 7.0
sigmoid_slope = 1.702


BLK = 512
NEG = -1e30
SMEM = pl.BlockSpec(memory_space=pltpu.SMEM)
VMEM = pl.BlockSpec(memory_space=pltpu.VMEM)
KEYS_FROM = (0, 7, 1, 6, 2, 5, 3, 4)


def pieces_of(values):
    high = values.astype(jnp.bfloat16).astype(jnp.float32)
    rest = values - high
    middle = rest.astype(jnp.bfloat16).astype(jnp.float32)
    return high, middle, rest - middle


def attend_kernel(first, place, *refs):
    q_refs, kv_refs = refs[:2], refs[2:10]
    gate_ref, near_ref, next_ref, kaug, vaug, qaug, held, acc, top, knorm = refs[10:]
    turn = pl.program_id(0)
    step = turn + first
    zed, ex = place[0], place[1]
    blocks = len(kv_refs)
    home = (ex - step) & 3
    half = BLK // 2

    @pl.when(turn == 0)
    def _prepare():
        one = jnp.ones((blocks, BLK), jnp.float32)
        rows = [jnp.zeros((64, BLK), jnp.float32)]
        spans = [
            gate_ref[:, pl.ds(pl.multiple_of((4 * b + ex) * BLK, BLK), BLK)] for b in range(blocks)
        ]
        for h in range(2):
            rows += list(pieces_of(-jnp.concatenate([span[h : h + 1] for span in spans], axis=0)))
        rows += [one, one]
        table = jnp.concatenate(rows, axis=0).T
        lane = lax.broadcasted_iota(jnp.int32, (BLK, 128), 1)
        tail = jnp.where(lax.broadcasted_iota(jnp.int32, (16, BLK), 0) == 0, 1.0, 0.0)
        most = jnp.zeros((1, BLK), jnp.float32)
        for kv_ref, away in zip(kv_refs, KEYS_FROM):
            b = (zed + away) & 7
            block = kv_ref[...].astype(jnp.float32)
            kaug[b] = jnp.where(
                lane < 64, block, jnp.where((lane & 7) == b, table, 0.0)
            ).astype(jnp.bfloat16)
            turned = block.T
            vaug[b] = jnp.concatenate([turned[64:], tail], axis=0).astype(jnp.bfloat16)
            keys = turned[:64]
            most = jnp.maximum(most, jnp.sum(keys * keys, axis=0, keepdims=True))
        knorm[0] = jnp.max(most)

    q_now = jnp.where(turn == 0, q_refs[0][...], q_refs[1][...])
    q_turned = q_now.astype(jnp.float32).T * 0.125
    q_most = jnp.maximum(
        jnp.max(jnp.sum(q_turned[:64] * q_turned[:64], axis=0, keepdims=True)),
        jnp.max(jnp.sum(q_turned[64:] * q_turned[64:], axis=0, keepdims=True)),
    )
    calm = q_most * knorm[0] <= 1600.0
    low_at = (4 * zed + home) * BLK
    high_at = (4 * (blocks - 1 - zed) + home) * BLK + half
    gates = jnp.concatenate(
        [gate_ref[:, pl.ds(pl.multiple_of(at, half), half)] for at in (low_at, high_at)], axis=1
    )
    for h in range(2):
        gate = gates[h : h + 1]
        high, low, _ = pieces_of(gate)
        on, off = jnp.ones((24, BLK), jnp.float32), jnp.zeros((24, BLK), jnp.float32)
        whole = jnp.concatenate(
            [
                q_turned[64 * h : 64 * h + 64],
                on if h == 0 else off,
                on if h == 1 else off,
                jnp.broadcast_to(high, (8, BLK)),
                jnp.broadcast_to(low, (8, BLK)),
            ],
            axis=0,
        ).astype(jnp.bfloat16)
        for part in range(2):
            qaug[part, h] = whole[:, part * half : part * half + half]
    acc[...] = jnp.zeros_like(acc)
    after = jnp.where(ex < home, 1, 0)
    low_count = zed + after
    count = blocks - 1 + 2 * after

    def unit(i):
        first = i < low_count
        return jnp.where(first, 0, 1), jnp.where(first, i, i - low_count)

    def scores_of(part, b, h):
        return jnp.dot(kaug[b], qaug[part, h], preferred_element_type=jnp.float32)

    def add(part, b, h, weights):
        acc[part, h] += jnp.dot(
            vaug[b], weights.astype(jnp.bfloat16), preferred_element_type=jnp.float32
        )

    def seen_of(part):
        return lax.broadcasted_iota(jnp.int32, (BLK, half), 0) <= (
            lax.broadcasted_iota(jnp.int32, (BLK, half), 1) + part * half
        )

    @pl.when(calm)
    def _calm():
        top[...] = jnp.zeros_like(top)
        part, b = unit(0)
        for h in range(2):
            held[h] = scores_of(part, b, h)

        def one(i, carry):
            part, b = unit(i)
            next_part, next_b = unit(jnp.minimum(i + 1, count - 1))
            for h in range(2):
                weights = jnp.exp(held[h])
                held[h] = scores_of(next_part, next_b, h)
                add(part, b, h, weights)
            return carry

        lax.fori_loop(0, count, one, 0)

        def edge(part):
            b = jnp.where(part == 0, zed, blocks - 1 - zed)
            for h in range(2):
                add(part, b, h, jnp.exp(jnp.where(seen_of(part), scores_of(part, b, h), NEG)))

        if first == 0:
            lax.fori_loop(0, jnp.where(turn == 0, 2, 0), lambda part, c: (edge(part), c)[1], 0)

    @pl.when(jnp.logical_not(calm))
    def _wild():
        top[...] = jnp.full_like(top, NEG)
        low_all = zed + jnp.where(ex <= home, 1, 0)

        def one(i, carry):
            h, n = i & 1, i >> 1
            part = jnp.where(n < low_all, 0, 1)
            b = n - part * low_all
            edge = (step == 0) & (b == jnp.where(part == 0, zed, blocks - 1 - zed))
            seen = seen_of(part + jnp.where(edge, 0, 4))
            scores = jnp.where(seen, scores_of(part, b, h), NEG)
            old = top[part, h]
            new = jnp.maximum(old, jnp.max(scores, axis=0, keepdims=True))
            top[part, h] = new
            acc[part, h] = acc[part, h] * jnp.exp(old - new)
            add(part, b, h, jnp.where(seen, jnp.exp(scores - new), 0.0))
            return carry

        lax.fori_loop(0, 2 * (blocks - 1 + 2 * jnp.where(ex <= home, 1, 0)), one, 0)

    for n, o_ref in enumerate((near_ref, next_ref)):

        @pl.when(turn == n)
        def _store(o_ref=o_ref):
            for h in range(2):
                for part in range(2):
                    rows = list(pieces_of(acc[part, h, 64:65])) + list(pieces_of(top[part, h]))
                    rows.append(jnp.zeros((10, half), jnp.float32))
                    o_ref[h, :, part * half : part * half + half] = jnp.concatenate(
                        [acc[part, h, :64]] + rows, axis=0
                    ).astype(jnp.bfloat16)


def attend(first, place, q_pair, kv_list, gates):
    n = len(kv_list)
    half = BLK // 2
    return pl.pallas_call(
        functools.partial(attend_kernel, first),
        grid_spec=pltpu.PrefetchScalarGridSpec(
            num_scalar_prefetch=1,
            grid=(2,),
            in_specs=[VMEM] * (3 + n),
            out_specs=[VMEM] * 2,
            scratch_shapes=[
                pltpu.VMEM((n, BLK, 128), jnp.bfloat16),
                pltpu.VMEM((n, 80, BLK), jnp.bfloat16),
                pltpu.VMEM((2, 2, 128, half), jnp.bfloat16),
                pltpu.VMEM((2, BLK, half), jnp.float32),
                pltpu.VMEM((2, 2, 80, half), jnp.float32),
                pltpu.VMEM((2, 2, 1, half), jnp.float32),
                pltpu.SMEM((1,), jnp.float32),
            ],
        ),
        out_shape=[jax.ShapeDtypeStruct((2, 80, BLK), jnp.bfloat16)] * 2,
        name="attend",
    )(place, *q_pair, *kv_list, gates)


def merge_kernel(*refs):
    parts, o_ref = refs[:4], refs[4]
    outs = []
    for h in range(2):
        peaks, totals = [], []
        for part in parts:
            side = part[h, 64:80].astype(jnp.float32)
            totals.append(side[0:1] + side[1:2] + side[2:3])
            peaks.append(side[3:4] + side[4:5] + side[5:6])
        peak = functools.reduce(jnp.maximum, peaks)
        factors = [jnp.exp(p - peak) for p in peaks]
        total = sum(f * t for f, t in zip(factors, totals))
        value = sum(f * part[h, :64].astype(jnp.float32) for part, f in zip(parts, factors))
        outs.append(value / total)
    o_ref[...] = jnp.concatenate(outs, axis=0).T.astype(jnp.bfloat16)


def merge(parts):
    return pl.pallas_call(
        merge_kernel,
        in_specs=[VMEM] * 4,
        out_specs=VMEM,
        out_shape=jax.ShapeDtypeStruct((BLK, 128), jnp.bfloat16),
        name="merge",
    )(*parts)


def project_kernel(place, *refs):
    pieces, (gain_ref, weight_ref, out_ref) = refs[:4], refs[4:]
    lefts = [piece[s].astype(jnp.float32) for piece in pieces for s in range(2)]
    order = [
        2 * ((place[2] - by) & 3) + (place[3] if s == 0 else 1 - place[3])
        for by in range(4)
        for s in range(2)
    ]
    squares = sum(jnp.sum(left * left, axis=1, keepdims=True) for left in lefts)
    inverse = lax.rsqrt(squares * (1.0 / 1024.0) + epsilon)
    total = None
    for j, left in zip(order, lefts):
        normed = (left * inverse * gain_ref[pl.ds(j, 1), :]).astype(jnp.bfloat16)
        rows = pl.ds(pl.multiple_of(j * 128, 128), 128)
        term = jnp.dot(normed, weight_ref[rows, :], preferred_element_type=jnp.float32)
        total = term if total is None else total + term
    out_ref[...] = total.astype(jnp.bfloat16)


def project(place, pieces, gain, weight):
    return pl.pallas_call(
        project_kernel,
        in_specs=[SMEM] + [VMEM] * 6,
        out_specs=VMEM,
        out_shape=jax.ShapeDtypeStruct((64, 2048), jnp.bfloat16),
        name="project",
    )(place, *pieces, gain.reshape(8, 128), weight)


def prepare_kernel(place, token_ref, gain_ref, route_ref, logit_ref, out_ref, table_ref):
    why, core = place[2], place[3]
    tokens = token_ref[...].astype(jnp.float32)
    rows, width = tokens.shape
    mean = jnp.sum(tokens * tokens, axis=1, keepdims=True) * (1.0 / width)
    columns = pl.ds(pl.multiple_of(why * 512, 512), 512)
    own = token_ref[:, columns].astype(jnp.float32)
    own = (own * lax.rsqrt(mean + epsilon) * gain_ref[:, columns]).astype(jnp.bfloat16)

    routes, logits = route_ref[...], logit_ref[...]
    raised = jnp.exp(logits - jnp.max(logits, axis=1, keepdims=True))
    weights = raised / jnp.sum(raised, axis=1, keepdims=True)
    number = lax.broadcasted_iota(jnp.int32, (rows, 32), 1)
    named = jnp.zeros((rows, 32), jnp.float32)
    share = jnp.zeros((rows, 32), jnp.float32)
    for k in range(4):
        same = routes[:, k : k + 1] == number
        named = jnp.where(same, 1.0, named)
        share = jnp.where(same, weights[:, k : k + 1], share)
    earlier = lax.broadcasted_iota(jnp.int32, (rows, rows), 0) > lax.broadcasted_iota(
        jnp.int32, (rows, rows), 1
    )
    slot = jnp.dot(
        jnp.where(earlier, 1.0, 0.0).astype(jnp.bfloat16),
        named.astype(jnp.bfloat16),
        preferred_element_type=jnp.float32,
    )
    position = lax.broadcasted_iota(jnp.int32, (32, 512), 1)
    widen = jnp.where(
        (position >> 4) == lax.broadcasted_iota(jnp.int32, (32, 512), 0), 1.0, 0.0
    ).astype(jnp.bfloat16)

    def widened(values):
        return jnp.dot(values.astype(jnp.bfloat16), widen, preferred_element_type=jnp.float32)

    wanted = (lax.broadcasted_iota(jnp.int32, (rows, 512), 1) & 15) + 16 * core + 1
    hit = widened(named * (slot + 1.0)) == wanted.astype(jnp.float32)
    onehot = jnp.where(hit, 1.0, 0.0)
    out_ref[...] = jnp.dot(
        onehot.T.astype(jnp.bfloat16), own, preferred_element_type=jnp.float32
    ).astype(jnp.bfloat16)
    high, low, _ = pieces_of(share)
    for n, piece in enumerate((high, low)):
        table_ref[n] = jnp.where(hit, widened(piece), 0.0).astype(jnp.bfloat16)


def prepare(place, tokens, gain, routes, logits):
    return pl.pallas_call(
        prepare_kernel,
        in_specs=[SMEM] + [VMEM] * 4,
        out_specs=[VMEM] * 2,
        out_shape=[
            jax.ShapeDtypeStruct((512, 512), jnp.bfloat16),
            jax.ShapeDtypeStruct((2, 128, 512), jnp.bfloat16),
        ],
        name="prepare",
    )(place, tokens, gain.reshape(1, -1), routes, logits)


def combine_kernel(place, table_ref, value_ref, keep_ref, send_ref):
    values = value_ref[...]
    total = sum(
        jnp.dot(table_ref[n], values, preferred_element_type=jnp.float32) for n in range(2)
    )
    first = place[3] == 0
    keep_ref[...] = jnp.where(first, total[:, :256], total[:, 256:])
    send_ref[...] = jnp.where(first, total[:, 256:], total[:, :256])


def combine(place, table, values):
    return pl.pallas_call(
        combine_kernel,
        in_specs=[SMEM] + [VMEM] * 2,
        out_specs=[VMEM] * 2,
        out_shape=[jax.ShapeDtypeStruct((128, 256), jnp.float32)] * 2,
        name="combine",
    )(place, table, values)


def experts_kernel(place, *refs):
    near, (top_ref, bottom_ref), weights = refs[:3], refs[3:5], refs[5:11]
    gates, ups, downs = weights[:2], weights[2:4], weights[4:]
    far_top, far_bottom, after_ref, before_ref, kept_ref = refs[11:]
    turn = pl.program_id(0)
    why = place[2]
    tile = pl.ds(pl.multiple_of(turn * 256, 256), 256)
    lefts = [piece[tile, :] for piece in near]
    lefts.append(jnp.where(turn == 0, top_ref[...], bottom_ref[...]))
    rows = [pl.ds(pl.multiple_of(((why - by) & 3) * 512, 512), 512) for by in (0, 1, 3, 2)]
    hidden = []
    for gate_ref, up_ref in zip(gates, ups):
        gate, up = (
            sum(
                jnp.dot(left, ref[row, :], preferred_element_type=jnp.float32)
                for left, row in zip(lefts, rows)
            )
            for ref in (gate_ref, up_ref)
        )
        gate = jnp.minimum(gate, clamp_limit)
        up = jnp.clip(up, -clamp_limit, clamp_limit)
        hidden.append(
            ((up + 1.0) * gate * jax.nn.sigmoid(sigmoid_slope * gate)).astype(jnp.bfloat16)
        )

    def partial(by):
        columns = pl.ds(pl.multiple_of(((why + by) & 3) * 512, 512), 512)
        return sum(
            jnp.dot(part, ref[:, columns], preferred_element_type=jnp.float32)
            for part, ref in zip(hidden, downs)
        ).astype(jnp.bfloat16)

    distant = partial(2)

    @pl.when(turn == 0)
    def _top():
        far_top[...] = distant

    @pl.when(turn == 1)
    def _bottom():
        far_bottom[...] = distant

    after_ref[tile, :] = partial(1)
    before_ref[tile, :] = partial(3)
    kept_ref[tile, :] = partial(0)


def experts(place, near, far, weights):
    shapes = [jax.ShapeDtypeStruct((n, 512), jnp.bfloat16) for n in (256, 256, 512, 512, 512)]
    return pl.pallas_call(
        experts_kernel,
        grid_spec=pltpu.PrefetchScalarGridSpec(
            num_scalar_prefetch=1,
            grid=(2,),
            in_specs=[VMEM] * 11,
            out_specs=[VMEM] * 5,
        ),
        out_shape=shapes,
        name="experts",
    )(place, *near, *far, *weights)


def shift(array, axis, by):
    count = lax.axis_size(axis)
    return lax.ppermute(array, axis, [(i, (i + by) % count) for i in range(count)])


def mirror(array):
    count = lax.axis_size("z")
    return lax.ppermute(array, "z", [(i, count - 1 - i) for i in range(count)])


def body(
    queries,
    keys_values,
    forget_cache,
    heads_gain,
    output_weight,
    expert_tokens,
    expert_gain,
    routes,
    route_logits,
    gate_weight,
    up_weight,
    down_weight,
):
    why, core = lax.axis_index("y"), lax.axis_index("c")
    place = jnp.stack([lax.axis_index("z"), lax.axis_index("x"), why, core]).astype(jnp.int32)
    middle = BLK // 2

    turned = mirror(queries[middle:])
    q = jnp.concatenate([queries[:middle], turned], axis=0)
    q_list = [q] + [shift(q, "x", by) for by in (1, 2, 3)]
    ups, downs = [keys_values], [keys_values]
    for _ in range(3):
        ups.append(shift(ups[-1], "z", 1))
    for _ in range(4):
        downs.append(shift(downs[-1], "z", 7))
    kv_list = [keys_values, ups[1], downs[1], ups[2], downs[2], ups[3], downs[3], downs[4]]

    outgoing, table = prepare(place, expert_tokens, expert_gain, routes, route_logits)
    arrived = lax.all_to_all(outgoing.reshape(32, 16, 512), EP, 0, 0, tiled=True)
    arrived = arrived.reshape(512, 512)
    weights = []
    for weight in (gate_weight[0], up_weight[0], down_weight[0]):
        weights += [weight, shift(weight, "c", 1)]
    left, right = shift(arrived, "y", 1), shift(arrived, "y", 3)
    far = [shift(left[:middle], "y", 1), shift(right[middle:], "y", 3)]
    top, bottom, after, before, kept = experts(place, [arrived, left, right], far, weights)
    first, second = shift(top, "y", 1), shift(bottom, "y", 3)

    def joined(a, b):
        return (a.astype(jnp.float32) + b.astype(jnp.float32)).astype(jnp.bfloat16)

    after = jnp.concatenate([joined(after[:middle], first), after[middle:]], axis=0)
    before = jnp.concatenate([before[:middle], joined(before[middle:], second)], axis=0)
    moved = [kept, shift(after, "y", 1)]
    moved.append(shift(before, "y", 3))
    expert_out = sum(m.astype(jnp.float32) for m in moved).astype(jnp.bfloat16)

    parts = attend(0, place, q_list[:2], kv_list, forget_cache)
    parts = [parts[0], shift(parts[1], "x", 3)]
    rest = attend(2, place, q_list[2:], kv_list, forget_cache)
    parts += [shift(rest[0], "x", 2), shift(rest[1], "x", 1)]
    returned = lax.all_to_all(expert_out.reshape(32, 16, 512), EP, 0, 0, tiled=True)
    attended = merge(parts)
    turned = mirror(attended[middle:])
    attended = jnp.concatenate([attended[:middle], turned], axis=0)
    attended = attended.reshape(4, 2, 64, 128)
    twin = shift(lax.dynamic_index_in_dim(attended, 1 - core, 1, keepdims=False), "c", 1)
    mine = lax.dynamic_index_in_dim(attended, core, 1, keepdims=False)
    both = jnp.stack([mine, twin], axis=1)
    slices = []
    for by in range(4):
        piece = lax.dynamic_index_in_dim(both, (why + by) & 3, 0, keepdims=False)
        slices.append(shift(piece, "y", by) if by else piece)
    mixer_out = project(place, slices, heads_gain, output_weight)

    keep, send = combine(place, table, returned.reshape(512, 512))
    moe_out = (keep + shift(send, "c", 1)).astype(jnp.bfloat16)
    return (mixer_out, moe_out)


def solution(mesh):
    torus = Mesh(mesh.devices.reshape(8, 4, 4, 2), ("z", "x", "y", "c"))
    return jax.shard_map(
        body,
        mesh=torus,
        in_specs=(
            P(EP, TP),
            P(EP, TP),
            P(TP, None),
            P(),
            P(),
            P(EP, None),
            P(),
            P(EP, None),
            P(EP, None),
            P(EP, None, TP),
            P(EP, None, TP),
            P(EP, TP, None),
        ),
        out_specs=(P(EP + TP, None), P(EP, TP)),
        check_vma=False,
    )
```

```python
import functools

import jax
import jax.numpy as jnp
from jax import lax
from jax.experimental import pallas as pl
from jax.experimental.pallas import tpu as pltpu
from jax.sharding import Mesh
from jax.sharding import PartitionSpec as P


EP = ("z", "x")
TP = ("y", "c")
epsilon = 1e-06
clamp_limit = 7.0
sigmoid_slope = 1.702


BLK = 512
NEG = -1e30
SMEM = pl.BlockSpec(memory_space=pltpu.SMEM)
VMEM = pl.BlockSpec(memory_space=pltpu.VMEM)
KEYS_FROM = (0, 7, 1, 6, 2, 5, 3, 4)


def near(array):
    return pltpu.with_memory_space_constraint(array, pltpu.VMEM)


def call(kernel, outs, place, *arrays, scratch=(), held=True):
    head = [] if place is None else [place]
    return pl.pallas_call(
        kernel,
        in_specs=[SMEM] * len(head) + [VMEM] * len(arrays),
        out_specs=[VMEM] * len(outs),
        out_shape=[(pltpu.VMEM if held else jax.ShapeDtypeStruct)(*out) for out in outs],
        scratch_shapes=scratch,
        compiler_params=pltpu.CompilerParams(vmem_limit_bytes=24 << 20),
    )(*head, *arrays)


def pieces_of(values):
    high = values.astype(jnp.bfloat16).astype(jnp.float32)
    rest = values - high
    middle = rest.astype(jnp.bfloat16).astype(jnp.float32)
    return high, middle, rest - middle


def attend_kernel(first, place, *refs):
    q_refs, kv_refs = refs[:2], refs[2:10]
    gate_ref, near_ref, next_ref, kaug, vaug, qaug, held, acc, top, knorm = refs[10:]
    zed, ex = place[0], place[1]
    blocks = len(kv_refs)
    half = BLK // 2

    one = jnp.ones((blocks, BLK), jnp.float32)
    rows = [jnp.zeros((64, BLK), jnp.float32)]
    spans = [
        gate_ref[:, pl.ds(pl.multiple_of((4 * b + ex) * BLK, BLK), BLK)] for b in range(blocks)
    ]
    for h in range(2):
        rows += list(pieces_of(jnp.concatenate([span[h : h + 1] for span in spans], axis=0)))
    rows += [one, one]
    table = jnp.concatenate(rows, axis=0).astype(jnp.bfloat16).T
    lane = lax.broadcasted_iota(jnp.int32, (BLK, 128), 1)
    is_key = jnp.where(lane < 64, 1.0, 0.0).astype(jnp.bfloat16)
    tail = jnp.where(lax.broadcasted_iota(jnp.int32, (16, BLK), 0) == 0, 1.0, 0.0)
    tail = tail.astype(jnp.bfloat16)
    key_rows = lax.broadcasted_iota(jnp.int32, (128, 128), 0) < 64
    key_rows = jnp.where(key_rows, 1.0, 0.0).astype(jnp.bfloat16)
    most = jnp.zeros((BLK, 128), jnp.float32)
    for kv_ref, away in zip(kv_refs, KEYS_FROM):
        b = (zed + away) & 7
        block = kv_ref[...]
        mine = jnp.where((lane & 7) == b, 1.0, 0.0).astype(jnp.bfloat16)
        kaug[b] = block * is_key + table * mine
        vaug[b, :64] = block.T[64:]
        vaug[b, 64:] = tail
        squares = jnp.dot(block * block, key_rows, preferred_element_type=jnp.float32)
        most = jnp.maximum(most, squares)
    knorm[0] = jnp.max(most)

    def take_turn(turn, carry):
        step = turn + first
        home = (ex - step) & 3
        q_now = jnp.where(turn == 0, q_refs[0][...], q_refs[1][...])
        q_turned = q_now.T.astype(jnp.float32) * 0.125
        squares = q_turned * q_turned
        q_most = jnp.max(
            jnp.maximum(
                jnp.sum(squares[:64], axis=0, keepdims=True),
                jnp.sum(squares[64:], axis=0, keepdims=True),
            )
        )
        calm = q_most * knorm[0] <= 1550.0
        low_at = (4 * zed + home) * BLK
        high_at = (4 * (blocks - 1 - zed) + home) * BLK + half
        gates = jnp.concatenate(
            [-gate_ref[:, pl.ds(pl.multiple_of(at, half), half)] for at in (low_at, high_at)], axis=1
        )
        for h in range(2):
            gate = gates[h : h + 1]
            high, low, _ = pieces_of(gate)
            on, off = jnp.ones((24, BLK), jnp.float32), jnp.zeros((24, BLK), jnp.float32)
            whole = jnp.concatenate(
                [
                    q_turned[64 * h : 64 * h + 64],
                    on if h == 0 else off,
                    on if h == 1 else off,
                    jnp.broadcast_to(high, (8, BLK)),
                    jnp.broadcast_to(low, (8, BLK)),
                ],
                axis=0,
            ).astype(jnp.bfloat16)
            for part in range(2):
                qaug[part, h] = whole[:, part * half : part * half + half]
        acc[...] = jnp.zeros_like(acc)
        after = jnp.where(ex < home, 1, 0)
        low_count = zed + after
        count = blocks - 1 + 2 * after

        def unit(i):
            first = i < low_count
            return jnp.where(first, 0, 1), jnp.where(first, i, i - low_count)

        def scores_of(part, b, h):
            return jnp.dot(kaug[b], qaug[part, h], preferred_element_type=jnp.float32)

        def add(part, b, h, weights):
            acc[part, h] += jnp.dot(
                vaug[b], weights.astype(jnp.bfloat16), preferred_element_type=jnp.float32
            )

        def seen_of(part):
            return lax.broadcasted_iota(jnp.int32, (BLK, half), 0) <= (
                lax.broadcasted_iota(jnp.int32, (BLK, half), 1) + part * half
            )

        @pl.when(calm)
        def _calm():
            top[...] = jnp.zeros_like(top)
            part, b = unit(0)
            for h in range(2):
                held[h] = jnp.exp(scores_of(part, b, h)).astype(jnp.bfloat16)

            def one(i, carry):
                part, b = unit(i)
                next_part, next_b = unit(jnp.minimum(i + 1, count - 1))
                for h in range(2):
                    weights = held[h]
                    held[h] = jnp.exp(scores_of(next_part, next_b, h)).astype(jnp.bfloat16)
                    add(part, b, h, weights)
                return carry

            lax.fori_loop(0, count, one, 0)

            def edge(part):
                b = jnp.where(part == 0, zed, blocks - 1 - zed)
                for h in range(2):
                    add(part, b, h, jnp.exp(jnp.where(seen_of(part), scores_of(part, b, h), NEG)))

            if first == 0:
                lax.fori_loop(0, jnp.where(turn == 0, 2, 0), lambda part, c: (edge(part), c)[1], 0)

        @pl.when(jnp.logical_not(calm))
        def _wild():
            top[...] = jnp.full_like(top, NEG)
            low_all = zed + jnp.where(ex <= home, 1, 0)

            def one(i, carry):
                h, n = i & 1, i >> 1
                part = jnp.where(n < low_all, 0, 1)
                b = n - part * low_all
                edge = (step == 0) & (b == jnp.where(part == 0, zed, blocks - 1 - zed))
                seen = seen_of(part + jnp.where(edge, 0, 4))
                scores = jnp.where(seen, scores_of(part, b, h), NEG)
                old = top[part, h]
                new = jnp.maximum(old, jnp.max(scores, axis=0, keepdims=True))
                top[part, h] = new
                acc[part, h] = acc[part, h] * jnp.exp(old - new)
                add(part, b, h, jnp.where(seen, jnp.exp(scores - new), 0.0))
                return carry

            lax.fori_loop(0, 2 * (blocks - 1 + 2 * jnp.where(ex <= home, 1, 0)), one, 0)

        for n, o_ref in enumerate((near_ref, next_ref)):

            @pl.when(turn == n)
            def _store(o_ref=o_ref):
                for h in range(2):
                    for part in range(2):
                        rows = list(pieces_of(acc[part, h, 64:65])) + list(pieces_of(top[part, h]))
                        rows.append(jnp.zeros((10, half), jnp.float32))
                        o_ref[h, :, part * half : part * half + half] = jnp.concatenate(
                            [acc[part, h, :64]] + rows, axis=0
                        ).astype(jnp.bfloat16)
        return carry

    lax.fori_loop(0, 2, take_turn, 0)


def attend(first, place, q_pair, kv_list, gates):
    n = len(kv_list)
    half = BLK // 2
    scratch = [
        pltpu.VMEM((n, BLK, 128), jnp.bfloat16),
        pltpu.VMEM((n, 80, BLK), jnp.bfloat16),
        pltpu.VMEM((2, 2, 128, half), jnp.bfloat16),
        pltpu.VMEM((2, BLK, half), jnp.bfloat16),
        pltpu.VMEM((2, 2, 80, half), jnp.float32),
        pltpu.VMEM((2, 2, 1, half), jnp.float32),
        pltpu.SMEM((1,), jnp.float32),
    ]
    outs = [((2, 80, BLK), jnp.bfloat16)] * 2
    kernel = functools.partial(attend_kernel, first)
    arrays = [near(array) for array in (*q_pair, *kv_list)]
    return call(kernel, outs, place, *arrays, gates, scratch=scratch)


def merge_kernel(*refs):
    parts, o_ref = refs[:4], refs[4]
    outs = []
    for h in range(2):
        peaks, totals = [], []
        for part in parts:
            side = part[h, 64:80].astype(jnp.float32)
            totals.append(side[0:1] + side[1:2] + side[2:3])
            peaks.append(side[3:4] + side[4:5] + side[5:6])
        peak = functools.reduce(jnp.maximum, peaks)
        factors = [jnp.exp(p - peak) for p in peaks]
        total = sum(f * t for f, t in zip(factors, totals))
        value = sum(f * part[h, :64].astype(jnp.float32) for part, f in zip(parts, factors))
        outs.append(value / total)
    o_ref[...] = jnp.concatenate(outs, axis=0).T.astype(jnp.bfloat16)


def merge(parts):
    return call(merge_kernel, [((BLK, 128), jnp.bfloat16)], None, *map(near, parts))[0]


def project_kernel(place, *refs):
    pieces, (gain_ref, weight_ref, out_ref) = refs[:4], refs[4:]
    lefts = [piece[s].astype(jnp.float32) for piece in pieces for s in range(2)]
    order = [
        2 * ((place[2] - by) & 3) + (place[3] if s == 0 else 1 - place[3])
        for by in range(4)
        for s in range(2)
    ]
    squares = sum(jnp.sum(left * left, axis=1, keepdims=True) for left in lefts)
    inverse = lax.rsqrt(squares * (1.0 / 1024.0) + epsilon)
    total = None
    for j, left in zip(order, lefts):
        normed = (left * inverse * gain_ref[pl.ds(j, 1), :]).astype(jnp.bfloat16)
        rows = pl.ds(pl.multiple_of(j * 128, 128), 128)
        term = jnp.dot(normed, weight_ref[rows, :], preferred_element_type=jnp.float32)
        total = term if total is None else total + term
    out_ref[...] = total.astype(jnp.bfloat16)


def project(place, pieces, gain, weight):
    outs = [((64, 2048), jnp.bfloat16)]
    arrays = [*map(near, pieces), gain.reshape(8, 128), weight]
    return call(project_kernel, outs, place, *arrays, held=False)[0]


def prepare_kernel(place, *refs):
    sources, (out_ref, table_ref), targets, arrivals = refs[:4], refs[4:6], refs[6:10], refs[10]
    copies = [
        pltpu.make_async_copy(source, target, arrivals.at[n])
        for n, (source, target) in enumerate(zip(sources, targets))
    ]
    for copy in copies:
        copy.start()
    for copy in copies:
        copy.wait()
    token_ref, gain_ref, route_ref, logit_ref = targets
    why, core = place[2], place[3]
    tokens = token_ref[...].astype(jnp.float32)
    rows, width = tokens.shape
    mean = jnp.sum(tokens * tokens, axis=1, keepdims=True) * (1.0 / width)
    columns = pl.ds(pl.multiple_of(why * 512, 512), 512)
    own = token_ref[:, columns].astype(jnp.float32)
    own = (own * lax.rsqrt(mean + epsilon) * gain_ref[:, columns]).astype(jnp.bfloat16)

    both = jnp.concatenate([route_ref[...].astype(jnp.float32), logit_ref[...]], axis=0).T
    routes, logits = both[:, :4].astype(jnp.int32), both[:, 4:]
    raised = jnp.exp(logits - jnp.max(logits, axis=1, keepdims=True))
    weights = raised / jnp.sum(raised, axis=1, keepdims=True)
    number = lax.broadcasted_iota(jnp.int32, (rows, 32), 1)
    named = jnp.zeros((rows, 32), jnp.float32)
    share = jnp.zeros((rows, 32), jnp.float32)
    for k in range(4):
        same = routes[:, k : k + 1] == number
        named = jnp.where(same, 1.0, named)
        share = jnp.where(same, weights[:, k : k + 1], share)
    earlier = lax.broadcasted_iota(jnp.int32, (rows, rows), 0) > lax.broadcasted_iota(
        jnp.int32, (rows, rows), 1
    )
    slot = jnp.dot(
        jnp.where(earlier, 1.0, 0.0).astype(jnp.bfloat16),
        named.astype(jnp.bfloat16),
        preferred_element_type=jnp.float32,
    )
    position = lax.broadcasted_iota(jnp.int32, (32, 512), 1)
    widen = jnp.where(
        (position >> 4) == lax.broadcasted_iota(jnp.int32, (32, 512), 0), 1.0, 0.0
    ).astype(jnp.bfloat16)

    def widened(values):
        return jnp.dot(values.astype(jnp.bfloat16), widen, preferred_element_type=jnp.float32)

    wanted = (lax.broadcasted_iota(jnp.int32, (rows, 512), 1) & 15) + 16 * core + 1
    hit = widened(named * (slot + 1.0)) == wanted.astype(jnp.float32)
    onehot = jnp.where(hit, 1.0, 0.0)
    out_ref[...] = jnp.dot(
        onehot.T.astype(jnp.bfloat16), own, preferred_element_type=jnp.float32
    ).astype(jnp.bfloat16)
    high, low, _ = pieces_of(share)
    for n, piece in enumerate((high, low)):
        table_ref[n] = jnp.where(hit, widened(piece), 0.0).astype(jnp.bfloat16)


def prepare(place, tokens, gain, routes, logits):
    arrays = [tokens, gain.reshape(1, -1), routes.T, logits.T]
    arrays = [pltpu.with_memory_space_constraint(array, pltpu.HBM) for array in arrays]
    outs = [((512, 512), jnp.bfloat16), ((2, 128, 512), jnp.bfloat16)]
    return pl.pallas_call(
        prepare_kernel,
        in_specs=[SMEM] + [pl.BlockSpec(memory_space=pltpu.HBM)] * 4,
        out_specs=[VMEM] * 2,
        out_shape=[pltpu.VMEM(*out) for out in outs],
        scratch_shapes=[pltpu.VMEM(array.shape, array.dtype) for array in arrays]
        + [pltpu.SemaphoreType.DMA((4,))],
        compiler_params=pltpu.CompilerParams(vmem_limit_bytes=24 << 20),
        name="prepare",
    )(place, *arrays)


def combine_kernel(place, table_ref, value_ref, keep_ref, send_ref):
    values = value_ref[...]
    total = sum(
        jnp.dot(table_ref[n], values, preferred_element_type=jnp.float32) for n in range(2)
    )
    first = place[3] == 0
    keep_ref[...] = jnp.where(first, total[:, :256], total[:, 256:])
    send_ref[...] = jnp.where(first, total[:, 256:], total[:, :256])


def combine(place, table, values):
    outs = [((128, 256), jnp.float32)] * 2
    return call(combine_kernel, outs, place, near(table), near(values))


def experts_kernel(place, *refs):
    close, (top_ref, bottom_ref), weights = refs[:3], refs[3:5], refs[5:11]
    gates, ups, downs = weights[:2], weights[2:4], weights[4:]
    outs, kept_ref = refs[11:17], refs[17]
    why = place[2]
    rows = [pl.ds(pl.multiple_of(((why - by) & 3) * 512, 512), 512) for by in (0, 1, 3, 2)]

    def take_turn(turn, carry):
        tile = pl.ds(pl.multiple_of(turn * 256, 256), 256)
        lefts = [piece[tile, :] for piece in close]
        lefts.append(jnp.where(turn == 0, top_ref[...], bottom_ref[...]))
        hidden = []
        for gate_ref, up_ref in zip(gates, ups):
            gate, up = (
                sum(
                    jnp.dot(left, ref[row, :], preferred_element_type=jnp.float32)
                    for left, row in zip(lefts, rows)
                )
                for ref in (gate_ref, up_ref)
            )
            gate = jnp.minimum(gate, clamp_limit)
            up = jnp.clip(up, -clamp_limit, clamp_limit)
            hidden.append(
                ((up + 1.0) * gate * jax.nn.sigmoid(sigmoid_slope * gate)).astype(jnp.bfloat16)
            )

        def partial(by):
            columns = pl.ds(pl.multiple_of(((why + by) & 3) * 512, 512), 512)
            return sum(
                jnp.dot(part, ref[:, columns], preferred_element_type=jnp.float32)
                for part, ref in zip(hidden, downs)
            ).astype(jnp.bfloat16)

        values = [partial(by) for by in (2, 1, 3)]
        for n in range(2):

            @pl.when(turn == n)
            def _store(n=n):
                for out, value in zip(outs[n::2], values):
                    out[...] = value

        kept_ref[tile, :] = partial(0)
        return carry

    lax.fori_loop(0, 2, take_turn, 0)


def experts(place, close, far, weights):
    outs = [((256, 512), jnp.bfloat16)] * 6 + [((512, 512), jnp.bfloat16)]
    return call(experts_kernel, outs, place, *map(near, (*close, *far, *weights)))


def join_kernel(*refs):
    for n in range(2):
        total = refs[n][...].astype(jnp.float32) + refs[n + 2][...].astype(jnp.float32)
        refs[n + 4][...] = total.astype(jnp.bfloat16)


def join(own, come):
    return call(join_kernel, [((256, 512), jnp.bfloat16)] * 2, None, *map(near, (*own, *come)))


def settle_kernel(kept_ref, *refs):
    parts, out_ref = refs[:4], refs[4]
    for n in range(2):
        tile = slice(256 * n, 256 * n + 256)
        total = sum(ref[...].astype(jnp.float32) for ref in parts[n::2])
        out_ref[tile, :] = (total + kept_ref[tile, :].astype(jnp.float32)).astype(jnp.bfloat16)


def settle(kept, parts):
    return call(settle_kernel, [((512, 512), jnp.bfloat16)], None, *map(near, (kept, *parts)))[0]


def shift(array, axis, by):
    count = lax.axis_size(axis)
    return lax.ppermute(array, axis, [(i, (i + by) % count) for i in range(count)])


def mirror(array):
    count = lax.axis_size("z")
    return lax.ppermute(array, "z", [(i, count - 1 - i) for i in range(count)])


def body(
    queries,
    keys_values,
    forget_cache,
    heads_gain,
    output_weight,
    expert_tokens,
    expert_gain,
    routes,
    route_logits,
    gate_weight,
    up_weight,
    down_weight,
):
    why, core = lax.axis_index("y"), lax.axis_index("c")
    place = jnp.stack([lax.axis_index("z"), lax.axis_index("x"), why, core]).astype(jnp.int32)
    middle = BLK // 2

    gates = near(-forget_cache)
    turned = mirror(queries[middle:])
    q = jnp.concatenate([queries[:middle], turned], axis=0)
    q_list = [q] + [shift(q, "x", by) for by in (1, 2, 3)]
    ups, downs = [keys_values], [keys_values]
    for _ in range(3):
        ups.append(shift(ups[-1], "z", 1))
    for _ in range(4):
        downs.append(shift(downs[-1], "z", 7))
    kv_list = [keys_values, ups[1], downs[1], ups[2], downs[2], ups[3], downs[3], downs[4]]

    outgoing, table = prepare(place, expert_tokens, expert_gain, routes, route_logits)
    arrived = lax.all_to_all(outgoing.reshape(32, 16, 512), EP, 0, 0, tiled=True)
    arrived = arrived.reshape(512, 512)
    weights = []
    for weight in (gate_weight[0], up_weight[0], down_weight[0]):
        weights += [weight, shift(weight, "c", 1)]
    left, right = shift(arrived, "y", 1), shift(arrived, "y", 3)
    far = [shift(left[:middle], "y", 1), shift(right[middle:], "y", 3)]
    top, bottom, after_top, after_bottom, before_top, before_bottom, kept = experts(
        place, [arrived, left, right], far, weights
    )
    first, second = shift(top, "y", 1), shift(bottom, "y", 3)
    low, high = shift(after_bottom, "y", 1), shift(before_top, "y", 3)
    after, before = join([after_top, before_bottom], [first, second])
    after, before = shift(after, "y", 1), shift(before, "y", 3)
    expert_out = settle(kept, [after, low, high, before])

    parts = attend(0, place, q_list[:2], kv_list, gates)
    parts = [parts[0], shift(parts[1], "x", 3)]
    rest = attend(2, place, q_list[2:], kv_list, gates)
    parts += [shift(rest[0], "x", 2), shift(rest[1], "x", 1)]
    returned = lax.all_to_all(expert_out.reshape(32, 16, 512), EP, 0, 0, tiled=True)
    attended = merge(parts)
    turned = mirror(attended[middle:])
    attended = jnp.concatenate([attended[:middle], turned], axis=0)
    attended = attended.reshape(4, 2, 64, 128)
    twin = shift(lax.dynamic_index_in_dim(attended, 1 - core, 1, keepdims=False), "c", 1)
    mine = lax.dynamic_index_in_dim(attended, core, 1, keepdims=False)
    both = jnp.stack([mine, twin], axis=1)
    slices = []
    for by in range(4):
        piece = lax.dynamic_index_in_dim(both, (why + by) & 3, 0, keepdims=False)
        slices.append(shift(piece, "y", by) if by else piece)
    mixer_out = project(place, slices, heads_gain, output_weight)

    keep, send = combine(place, table, returned.reshape(512, 512))
    moe_out = (keep + shift(send, "c", 1)).astype(jnp.bfloat16)
    return (mixer_out, moe_out)


def solution(mesh):
    torus = Mesh(mesh.devices.reshape(8, 4, 4, 2), ("z", "x", "y", "c"))
    return jax.shard_map(
        body,
        mesh=torus,
        in_specs=(
            P(EP, TP),
            P(EP, TP),
            P(TP, None),
            P(),
            P(),
            P(EP, None),
            P(),
            P(EP, None),
            P(EP, None),
            P(EP, None, TP),
            P(EP, None, TP),
            P(EP, TP, None),
        ),
        out_specs=(P(EP + TP, None), P(EP, TP)),
        check_vma=False,
    )
```
